256 devices in a mesh: grp: 2 (over y), ep: 64 (over z, x), tp: 2 (over core).
Axes of the slice: x: 4, y: 2, z: 16, core: 2. Of those that a mesh axis runs over, the one named last changes fastest.
The devices are a block of a 4x16x16 slice.
Arguments:
- tokens: bfloat16 [12288, 2048], P(('grp', 'ep')), parts along dimension 0, may hold values from -6 to 6
- prior_state: float32 [2, 12288, 4096], P(None, ('grp', 'ep'), 'tp'), parts along dimension 1, may hold values from -6 to 6
- mix_gain: float32 [2048], replicated, may hold values from 0.1 to 1.9
- in_weight: bfloat16 [2048, 1024], P(None, 'tp'), may hold values from -0.125 to 0.125
- decay_rate: float32 [64, 64], P('tp'), may hold values from 0.2 to 20
- frequency: float32 [64, 64], P('tp'), may hold values from 0 to 12
- log_step: float32 [64], P('tp'), may hold values from -4.6 to 0
- input_map: float32 [2, 64, 64, 16], P(None, 'tp'), may hold values from -6 to 6
- output_map: float32 [2, 64, 16, 64], P(None, 'tp'), may hold values from -0.5 to 0.5
- skip_gain: float32 [1024], P('tp'), may hold values from -4 to 4
- out_weight: bfloat16 [1024, 2048], P('tp'), may hold values from -0.1875 to 0.1875
- channel_gain: float32 [2048], replicated, may hold values from 0.1 to 1.9
- expert_gate: bfloat16 [64, 2048, 512], P('ep', None, 'tp'), may hold values from -0.125 to 0.125
- expert_up: bfloat16 [64, 2048, 512], P('ep', None, 'tp'), may hold values from -0.125 to 0.125
- expert_down: bfloat16 [64, 512, 2048], P('ep', 'tp'), may hold values from -0.25 to 0.25
- shared_gate: bfloat16 [2048, 512], P(None, 'tp'), may hold values from -0.125 to 0.125
- shared_up: bfloat16 [2048, 512], P(None, 'tp'), may hold values from -0.125 to 0.125
- shared_down: bfloat16 [512, 2048], P('tp'), may hold values from -0.25 to 0.25
- routes: int32 [12288, 6], P(('grp', 'ep')), parts along dimension 0, may hold values from 0 to 63, all different within a row; in each aligned block of 96 rows (0 to 95, 96 to 191, ...) at most 13 rows name the same one
- route_weights: float32 [12288, 6], P(('grp', 'ep')), parts along dimension 0, may hold values from 0.05 to 0.8
Outputs:
- layer_out: bfloat16 [12288, 2048], P(('grp', 'ep'), 'tp'), parts along dimension 0
- new_state: float32 [2, 12288, 4096], P(None, ('grp', 'ep'), 'tp'), parts along dimension 1
The draws below stay inside these ranges and needn't reach their ends.
There are 2 independent parts, one for each index of `grp`. The reference program is written for one: setup_inputs(seed, part) draws one part's arguments, and reference() takes and returns one part's arrays. A program takes and returns all parts, laid end to end along the dimension named above; an argument that names none is the same for every part. Nothing has to cross between parts.
Inputs may be any that keep to these rules, and one draw needn't show every extreme that they name: `routes`: each row names 6 different experts; among the rows of one index of ep no expert is named by more than 13 rows.
All inputs are finite; a program needn't handle non-finite values.
Results may differ from the reference program's by a relative error of at most 0.017.
Values may be sent and summed in bfloat16 or wider, within the bound.
No kernel may reach another device: no remote copies, remote signals or barrier semaphores. Data moves between devices by JAX's collectives and lax.ppermute only.
A program may use at most 128 MiB of HBM per device.

```python
import math
import jax
import jax.numpy as jnp
import numpy as np
from jax import lax

D = 2048
SSM_WIDTH = 1024
GROUPS = 64
GROUP_WIDTH = 16
STATE = 64
EXP_WIDTH = 512
SHARED_WIDTH = 512
TOPK = 6
SEQ_DEV = 96
SEQS = 6144
EXPERTS = 64
CAP = 13
N_EP = 64
N_TP = 2


def block_levels(stream_key, extent, pieces, smallest, high):
    def one(position, blocks):
        heights = jax.random.uniform(jax.random.fold_in(jax.random.fold_in(stream_key, 6), position), (blocks,), jnp.float32, smallest / len(pieces), high / len(pieces))
        return jnp.repeat(jnp.exp(heights), extent[position] // blocks).reshape((-1,) + (1,) * (len(extent) - position - 1))

    factor_of = one(*pieces[0])
    for cut in pieces[1:]:
        factor_of = factor_of * one(*cut)
    return factor_of


def deal_out(rng, own, number, rows, number_of, top, reach, skew):
    order = jax.random.permutation(rng, number_of)
    packed, ordinary = shares(number_of, rows * top, reach, skew, True), shares(number_of, rows * top, reach, skew, False)
    places = jnp.arange(number_of)

    def named(sizes, offset_by):
        used = int((sizes > 0).sum())
        fixed = max(1, used // 4)
        passed = fixed + (places - fixed + offset_by * (used - fixed)) % max(1, number_of - fixed)
        return jnp.zeros((number_of,), jnp.int32).at[order[jnp.where(places < fixed, places, passed)]].set(jnp.asarray(sizes, jnp.int32))

    sizes = jnp.where(number % 4 == 0, named(packed, number // 4), named(ordinary, number - number // 4 - 1))
    mixed = jax.random.permutation(jax.random.fold_in(own, 3), number_of)
    donor, receiver = mixed[0:number_of // 2 * 2:2], mixed[1:number_of // 2 * 2:2]
    margin = jnp.minimum(sizes[donor] - 1, reach - sizes[receiver]) // 2
    margin = jnp.where((donor == order[0]) | (receiver == order[0]) | (sizes[receiver] == 0), 0, jnp.maximum(margin, 0))
    passed = jax.random.randint(jax.random.fold_in(own, 4), (number_of // 2,), 0, 1 << 20) % (margin + 1)
    sizes = sizes.at[donor].add(-passed).at[receiver].add(passed)
    labels = jnp.searchsorted(jnp.cumsum(sizes), jnp.arange(rows * top), side="right").astype(jnp.int32)
    grid = labels.reshape(top, rows).T
    grid = grid[jax.random.permutation(jax.random.fold_in(own, 1), rows)]
    offset_by = jax.random.randint(jax.random.fold_in(own, 2), (rows, 1), 0, top)
    return jnp.take_along_axis(grid, (jnp.arange(top)[None, :] + offset_by) % top, axis=1)


def shares(amount, total, reach, slope, full):
    weights = [(1 << 20) // math.isqrt(rank ** slope) + 1 for rank in range(1, amount + 1)]
    largest = reach if full else min(reach, max(-(-total // amount), total * weights[0] // sum(weights)))
    least = 1 if total - largest >= amount - 1 else 0
    counts, spare = [largest] + [least] * (amount - 1), total - largest - least * (amount - 1)
    while spare > 0:
        free = [i for i in range(1, amount) if counts[i] < largest] or [i for i in range(1, amount) if counts[i] < reach]
        mass, left = sum([weights[i] for i in free]), spare
        for i in free:
            more = min(reach - counts[i], max(1, left * weights[i] // mass), spare)
            counts[i] = counts[i] + more
            spare = spare - more
    return np.array(counts)


def gaussian(key, dims, spread, most, shards=(), held_as=jnp.bfloat16):
    drawn = spread * jax.random.normal(key, dims, jnp.float32)
    if shards:
        drawn = drawn * block_levels(key, dims, shards, -0.22, 0.18)
    return jnp.clip(drawn, -most, most).astype(held_as)


def setup_inputs(seed: int = 0, part: int = 0) -> dict:
    keys = jax.random.split(jax.random.key(seed), 21)
    part_keys = jax.random.split(jax.random.fold_in(keys[20], part), 21)
    tokens = gaussian(part_keys[0], (SEQS, D), 1.0, 6.0, ((0, 64),))
    prior_state = gaussian(part_keys[1], (2, SEQS, GROUPS * STATE), 1.0, 6.0, ((1, 64), (2, 2)), jnp.float32)
    mix_gain = jnp.clip(1.0 + 0.18 * jax.random.normal(keys[2], (D,), jnp.float32), 0.1, 1.9)
    in_weight = gaussian(keys[3], (D, SSM_WIDTH), D ** -0.5, 0.125, ((1, 2),))
    decay_rate = jnp.clip(jnp.exp(math.log(20.0) - 4.6051702 * jax.random.uniform(keys[4], (GROUPS, STATE), jnp.float32) ** block_levels(keys[4], (GROUPS, STATE), ((0, 2),), -0.2, 0.2)), 0.2, 20.0)
    frequency = jnp.clip(12.0 * jax.random.uniform(keys[5], (GROUPS, STATE), jnp.float32) ** block_levels(keys[5], (GROUPS, STATE), ((0, 2),), -0.2, 0.2), 0.0, 12.0)
    log_step = jnp.clip(-4.6 + 4.6 * jax.random.uniform(keys[6], (GROUPS,), jnp.float32) ** block_levels(keys[6], (GROUPS,), ((0, 2),), -0.2, 0.2), -4.6, 0.0)
    input_map = gaussian(keys[7], (2, GROUPS, STATE, GROUP_WIDTH), 1.0, 6.0, ((1, 2),), jnp.float32)
    output_map = gaussian(keys[8], (2, GROUPS, GROUP_WIDTH, STATE), (2 * STATE) ** -0.5, 0.5, ((1, 2),), jnp.float32)
    skip_gain = gaussian(keys[9], (SSM_WIDTH,), 1.0, 4.0, ((0, 2),), jnp.float32)
    out_weight = gaussian(keys[10], (SSM_WIDTH, D), SSM_WIDTH ** -0.5, 0.1875, ((0, 2),))
    channel_gain = jnp.clip(1.0 + 0.18 * jax.random.normal(keys[11], (D,), jnp.float32), 0.1, 1.9)
    expert_gate = gaussian(keys[12], (EXPERTS, D, EXP_WIDTH), D ** -0.5, 0.125, ((0, 64), (2, 2)))
    expert_up = gaussian(keys[13], (EXPERTS, D, EXP_WIDTH), D ** -0.5, 0.125, ((0, 64), (2, 2)))
    expert_down = gaussian(keys[14], (EXPERTS, EXP_WIDTH, D), EXP_WIDTH ** -0.5, 0.25, ((0, 64), (1, 2)))
    shared_gate = gaussian(keys[15], (D, SHARED_WIDTH), D ** -0.5, 0.125, ((1, 2),))
    shared_up = gaussian(keys[16], (D, SHARED_WIDTH), D ** -0.5, 0.125, ((1, 2),))
    shared_down = gaussian(keys[17], (SHARED_WIDTH, D), SHARED_WIDTH ** -0.5, 0.25, ((0, 2),))
    routes_keys = jax.random.split(jax.random.fold_in(part_keys[18], 1), SEQS // SEQ_DEV)
    routes_turns = jax.random.permutation(jax.random.fold_in(part_keys[18], 3), SEQS // SEQ_DEV)
    routes = jax.vmap(lambda own, number: deal_out(jax.random.fold_in(part_keys[18], 2), own, number, SEQ_DEV, EXPERTS, TOPK, CAP, 2))(routes_keys, routes_turns).reshape((SEQS, TOPK))
    route_weights = jnp.clip(0.05 + 0.75 * jax.random.uniform(part_keys[19], (SEQS, TOPK), jnp.float32) ** block_levels(part_keys[19], (SEQS, TOPK), ((0, 64),), -0.2, 0.2), 0.05, 0.8)
    return {"tokens": tokens, "prior_state": prior_state, "mix_gain": mix_gain, "in_weight": in_weight, "decay_rate": decay_rate, "frequency": frequency, "log_step": log_step, "input_map": input_map, "output_map": output_map, "skip_gain": skip_gain, "out_weight": out_weight, "channel_gain": channel_gain, "expert_gate": expert_gate, "expert_up": expert_up, "expert_down": expert_down, "shared_gate": shared_gate, "shared_up": shared_up, "shared_down": shared_down, "routes": routes, "route_weights": route_weights}


norm_eps = 1e-06
highest = lax.Precision.HIGHEST

def root_scale(activations, scale_gain):
    values = activations.astype(jnp.float32)
    factor = lax.rsqrt(lax.optimization_barrier(jnp.mean(values * values, axis=-1, keepdims=True)) + norm_eps)
    return (values * factor * scale_gain).astype(jnp.bfloat16)

def state_update(drive_rows, prior_state, decay_rate, frequency, log_step, input_map, output_map, skip_gain):
    sequences = drive_rows.shape[0]
    groups = decay_rate.shape[0]
    driven = drive_rows.astype(jnp.float32).reshape(sequences, groups, -1)
    step_size = jnp.exp(log_step)[:, None]
    real_rate = -decay_rate
    magnitude = jnp.exp(real_rate * step_size)
    turn_real = magnitude * jnp.cos(frequency * step_size)
    turn_imag = magnitude * jnp.sin(frequency * step_size)
    denominator = real_rate * real_rate + frequency * frequency
    hold_real = ((turn_real - 1.0) * real_rate + turn_imag * frequency) / denominator
    hold_imag = (turn_imag * real_rate - (turn_real - 1.0) * frequency) / denominator
    push_real = jnp.einsum('sgh,gph->sgp', driven, input_map[0], precision=highest)
    push_imag = jnp.einsum('sgh,gph->sgp', driven, input_map[1], precision=highest)
    enter_real = push_real * hold_real - push_imag * hold_imag
    enter_imag = push_real * hold_imag + push_imag * hold_real
    old_real = prior_state[0].reshape(sequences, groups, -1)
    old_imag = prior_state[1].reshape(sequences, groups, -1)
    fresh_real = turn_real * old_real - turn_imag * old_imag + enter_real
    fresh_imag = turn_real * old_imag + turn_imag * old_real + enter_imag
    readout = jnp.einsum('ghp,sgp->sgh', output_map[0], fresh_real, precision=highest)
    readout = readout - jnp.einsum('ghp,sgp->sgh', output_map[1], fresh_imag, precision=highest)
    readout = readout.reshape(sequences, -1) + skip_gain * drive_rows.astype(jnp.float32)
    fresh = jnp.stack([fresh_real.reshape(sequences, -1), fresh_imag.reshape(sequences, -1)])
    return (readout, fresh)

def split_block(activations, gate_weight, up_weight, down_weight):
    col_width = gate_weight.shape[1] // N_TP
    summed = jnp.zeros((activations.shape[0], down_weight.shape[1]), jnp.float32)
    for portion in range(N_TP):
        lower = portion * col_width
        gate_val = jnp.dot(activations, gate_weight[:, lower:lower + col_width], preferred_element_type=jnp.float32)
        up_val = jnp.dot(activations, up_weight[:, lower:lower + col_width], preferred_element_type=jnp.float32)
        hidden = (jax.nn.silu(gate_val) * up_val).astype(jnp.bfloat16)
        piece = jnp.dot(hidden, down_weight[lower:lower + col_width], preferred_element_type=jnp.float32)
        summed = summed + lax.optimization_barrier(piece.astype(jnp.bfloat16)).astype(jnp.float32)
    return summed

def reference(tokens, prior_state, mix_gain, in_weight, decay_rate, frequency, log_step, input_map, output_map, skip_gain, out_weight, channel_gain, expert_gate, expert_up, expert_down, shared_gate, shared_up, shared_down, routes, route_weights):
    normed = root_scale(tokens, mix_gain)
    drive_rows = jnp.dot(normed, in_weight, preferred_element_type=jnp.float32).astype(jnp.bfloat16)
    readout, new_state = state_update(drive_rows, prior_state, decay_rate, frequency, log_step, input_map, output_map, skip_gain)
    activated = jax.nn.gelu(readout).astype(jnp.bfloat16)
    col_width = out_weight.shape[0] // N_TP
    mixer_out = jnp.zeros((SEQS, D), jnp.float32)
    for portion in range(N_TP):
        lower = portion * col_width
        piece = jnp.dot(activated[:, lower:lower + col_width], out_weight[lower:lower + col_width], preferred_element_type=jnp.float32)
        mixer_out = mixer_out + lax.optimization_barrier(piece.astype(jnp.bfloat16)).astype(jnp.float32)
    middle = (tokens.astype(jnp.float32) + mixer_out).astype(jnp.bfloat16)
    second_normed = root_scale(middle, channel_gain)
    shared_out = split_block(second_normed, shared_gate, shared_up, shared_down)
    slot_limit = N_EP * CAP
    flat_routes = routes.reshape(-1)
    flat_weights = route_weights.reshape(-1)

    def one_expert(running, operands):
        expert_id, gate_weight, up_weight, down_weight = operands
        matched = flat_routes == expert_id
        chosen = jnp.nonzero(matched, size=slot_limit, fill_value=0)[0].astype(jnp.int32)
        found_count = jnp.sum(matched.astype(jnp.int32))
        is_valid = jnp.arange(slot_limit, dtype=jnp.int32) < found_count
        row_index = chosen // TOPK
        picked_rows = jnp.take(second_normed, row_index, axis=0)
        produced = split_block(picked_rows, gate_weight, up_weight, down_weight).astype(jnp.bfloat16)
        produced = lax.optimization_barrier(produced).astype(jnp.float32)
        weight_vals = jnp.where(is_valid, jnp.take(flat_weights, chosen), jnp.zeros_like(flat_weights[:1]))
        running = running.at[row_index].add(weight_vals[:, None] * produced)
        return (running, None)
    routed, _ = lax.scan(one_expert, jnp.zeros((SEQS, D), jnp.float32), (jnp.arange(EXPERTS, dtype=jnp.int32), expert_gate, expert_up, expert_down))
    layer_out = (middle.astype(jnp.float32) + routed + shared_out).astype(jnp.bfloat16)
    return (layer_out, new_state)
```

```python
import jax
import jax.numpy as jnp
from jax import lax
from jax.experimental import pallas as pl
from jax.experimental.pallas import tpu as pltpu
from jax.sharding import PartitionSpec as P

norm_eps = 1e-06
RING = 4
NEAR = 4
AXES = ("ep", "tp")
f32, bf16 = jnp.float32, jnp.bfloat16
BIG = pltpu.CompilerParams(vmem_limit_bytes=56 * 1024 * 1024)
VM = pl.BlockSpec(memory_space=pltpu.VMEM)
SM = pl.BlockSpec(memory_space=pltpu.SMEM)


def dot(a, b):
    return jnp.dot(a, b, preferred_element_type=f32)


def scaled(values, gain):
    factor = lax.rsqrt(jnp.mean(values * values, axis=-1, keepdims=True) + norm_eps)
    return (values * factor * gain).astype(bf16)


def mixer_kernel(tok, gain, w_in, state, coef, imap, omap, skip, w_out, fresh, partial, normed, acc):
    step = pl.program_id(0)

    @pl.when(step == 0)
    def _():
        normed[...] = scaled(tok[...].astype(f32), gain[...])

    drive = dot(normed[...], w_in[...]).astype(bf16)
    chans, entries = imap.shape[1], imap.shape[2]
    groups = coef.shape[1]
    width, wide = chans // groups, groups * entries
    same = (lax.broadcasted_iota(jnp.int32, (chans, wide), 0) // width) == (
        lax.broadcasted_iota(jnp.int32, (chans, wide), 1) // entries
    )

    def spread(m):
        return jnp.where(same, jnp.concatenate([m] * groups, axis=1), 0.0).astype(bf16)

    def row(m):
        return jnp.concatenate([m[g : g + 1, :] for g in range(groups)], axis=1)

    push_re, push_im = dot(drive, spread(imap[0])), dot(drive, spread(imap[1]))
    turn_re, turn_im, hold_re, hold_im = [row(coef[i]) for i in range(4)]
    old_re, old_im = state[0], state[1]
    new_re = turn_re * old_re - turn_im * old_im + (push_re * hold_re - push_im * hold_im)
    new_im = turn_re * old_im + turn_im * old_re + (push_re * hold_im + push_im * hold_re)
    fresh[0] = new_re
    fresh[1] = new_im
    nt = (((1,), (1,)), ((), ()))
    readout = lax.dot_general(
        new_re.astype(bf16), spread(omap[0]), nt, preferred_element_type=f32
    ) - lax.dot_general(new_im.astype(bf16), spread(omap[1]), nt, preferred_element_type=f32)
    readout = readout + skip[...] * drive.astype(f32)
    part = dot(jax.nn.gelu(readout).astype(bf16), w_out[...])

    @pl.when(step == 0)
    def _():
        acc[...] = part

    @pl.when(step > 0)
    def _():
        acc[...] += part

    @pl.when(step == pl.num_programs(0) - 1)
    def _():
        partial[...] = acc[...].astype(bf16)


def mixer(tokens, gain, w_in, state, coef, imap, omap, skip, w_out):
    rows, width = tokens.shape
    chans = w_in.shape[1]
    groups, entries = coef.shape[1:]
    steps = 4
    c, g, s = chans // steps, groups // steps, groups * entries // steps
    return pl.pallas_call(
        mixer_kernel,
        grid=(steps,),
        in_specs=[
            pl.BlockSpec((rows, width), lambda i: (0, 0)),
            pl.BlockSpec((1, width), lambda i: (0, 0)),
            pl.BlockSpec((width, c), lambda i: (0, i)),
            pl.BlockSpec((2, rows, s), lambda i: (0, 0, i)),
            pl.BlockSpec((4, g, entries), lambda i: (0, i, 0)),
            pl.BlockSpec((2, c, entries), lambda i: (0, i, 0)),
            pl.BlockSpec((2, c, entries), lambda i: (0, i, 0)),
            pl.BlockSpec((1, c), lambda i: (0, i)),
            pl.BlockSpec((c, width), lambda i: (i, 0)),
        ],
        out_specs=[
            pl.BlockSpec((2, rows, s), lambda i: (0, 0, i)),
            pl.BlockSpec((rows, width), lambda i: (0, 0)),
        ],
        out_shape=[
            jax.ShapeDtypeStruct(state.shape, f32),
            jax.ShapeDtypeStruct((rows, width), bf16),
        ],
        scratch_shapes=[pltpu.VMEM((rows, width), bf16), pltpu.VMEM((rows, width), f32)],
        compiler_params=BIG,
        name="mixer",
    )(tokens, gain, w_in, state, coef, imap, omap, skip, w_out)


def turn_and_hold(decay_rate, frequency, log_step):
    step_size = jnp.exp(log_step)[:, None]
    real_rate = -decay_rate
    magnitude = jnp.exp(real_rate * step_size)
    turn_real = magnitude * jnp.cos(frequency * step_size)
    turn_imag = magnitude * jnp.sin(frequency * step_size)
    denominator = real_rate * real_rate + frequency * frequency
    hold_real = ((turn_real - 1.0) * real_rate + turn_imag * frequency) / denominator
    hold_imag = (turn_imag * real_rate - (turn_real - 1.0) * frequency) / denominator
    return jnp.stack([turn_real, turn_imag, hold_real, hold_imag])


def second_norm_kernel(core, tok, mine, other, gain, own_half, far_half, mid_half, normed, mid):
    middle = (tok[...].astype(f32) + (mine[...].astype(f32) + other[...].astype(f32))).astype(bf16)
    mid[...] = middle
    normed[...] = scaled(middle.astype(f32), gain[...])
    half = own_half.shape[1]
    here = pl.multiple_of(core[0] * half, half)
    there = pl.multiple_of((1 - core[0]) * half, half)
    own_half[...] = normed[:, pl.ds(here, half)]
    far_half[...] = normed[:, pl.ds(there, half)]
    mid_half[...] = mid[:, pl.ds(here, half)]


def second_norm(core, tokens, mine, other, gain):
    rows, width = tokens.shape
    piece = jax.ShapeDtypeStruct((rows, width // 2), bf16)
    return pl.pallas_call(
        second_norm_kernel,
        in_specs=[SM, VM, VM, VM, VM],
        out_specs=[VM, VM, VM],
        out_shape=[piece, piece, piece],
        scratch_shapes=[pltpu.VMEM((rows, width), bf16), pltpu.VMEM((rows, width), bf16)],
        compiler_params=BIG,
        name="second_norm",
    )(core, tokens, mine, other, gain)


def block_kernel(core, own, other, gate, up, down, keep, send):
    half = own.shape[1]
    here = pl.multiple_of(core[0] * half, half)
    there = pl.multiple_of((1 - core[0]) * half, half)
    a, b = own[...], other[...]
    gate_val = dot(a, gate[pl.ds(here, half), :]) + dot(b, gate[pl.ds(there, half), :])
    up_val = dot(a, up[pl.ds(here, half), :]) + dot(b, up[pl.ds(there, half), :])
    hidden = (jax.nn.silu(gate_val) * up_val).astype(bf16)
    send[...] = dot(hidden, down[:, pl.ds(there, half)]).astype(bf16)
    keep[...] = dot(hidden, down[:, pl.ds(here, half)]).astype(bf16)


def block(core, own, other, gate, up, down, tile):
    rows, half = own.shape
    whole = lambda a: pl.BlockSpec(a.shape, lambda i: (0, 0))
    strip = pl.BlockSpec((tile, half), lambda i: (i, 0))
    piece = jax.ShapeDtypeStruct((rows, half), bf16)
    return pl.pallas_call(
        block_kernel,
        grid=(rows // tile,),
        in_specs=[SM, strip, strip, whole(gate), whole(up), whole(down)],
        out_specs=[strip, strip],
        out_shape=[piece, piece],
        compiler_params=BIG,
        name="block",
    )(core, own, other, gate, up, down)


def place_kernel(info, r0, r1, r2, r3, pick, mix):
    plane, core, base = info[0], info[1], info[2]
    planes, cap = info[3], info[4]
    dests, slots = NEAR * RING, pick.shape[1] // (NEAR * RING)
    rows = pick.shape[2]
    top = r0.shape[0] // 2
    order = lax.broadcasted_iota(jnp.int32, (dests, 1), 0)
    near, across = order // RING, order % RING
    spot = base + near - jnp.where(near >= NEAR // 2, NEAR * core, 0)
    spot = jnp.where(spot < 0, spot + planes, spot)
    expert = (spot * RING + across).astype(f32)
    before = lax.broadcasted_iota(jnp.int32, (rows, rows), 0) < lax.broadcasted_iota(
        jnp.int32, (rows, rows), 1
    )
    before = before.astype(f32).astype(bf16)
    level = lax.broadcasted_iota(jnp.int32, (slots, rows), 0).astype(f32)
    for m, ref in enumerate((r0, r1, r2, r3)):
        table = ref[...]
        hits = jnp.zeros((dests, rows), f32)
        weight = jnp.zeros((dests, rows), f32)
        for k in range(top):
            hit = (table[k : k + 1, :] == expert).astype(f32)
            hits = hits + hit
            weight = weight + hit * table[top + k : top + k + 1, :]
        rank = dot(hits.astype(bf16), before)
        home = plane - NEAR * m
        home = jnp.where(home < 0, home + planes, home) // NEAR
        place = jnp.where(hits > 0.5, rank + (home * cap).astype(f32), -1.0)
        for d in range(0, dests, 2):
            ones = [(level == place[e : e + 1, :]).astype(f32) for e in (d, d + 1)]
            mixed = [one * weight[e : e + 1, :] for one, e in zip(ones, (d, d + 1))]
            span = pl.ds(d * slots, 2 * slots)
            pick[m, span, :] = jnp.concatenate(ones, axis=0).astype(bf16)
            mix[m, span, :] = jnp.concatenate(mixed, axis=0).astype(bf16)


def place(info, tables, slots):
    rows = tables[0].shape[1]
    shape = jax.ShapeDtypeStruct((4, NEAR * RING * slots, rows), bf16)
    return pl.pallas_call(
        place_kernel,
        in_specs=[SM, VM, VM, VM, VM],
        out_specs=[VM, VM],
        out_shape=[shape, shape],
        compiler_params=BIG,
        name="place",
    )(info, *tables)


def pick_kernel(pick, own, below, far_a, far_b, above, out):
    total = pick.shape[1]
    half = far_a.shape[1]
    tile = 128
    for i in range(total // tile):
        span = pl.ds(i * tile, tile)
        rest = (
            dot(pick[0, span, :], own[...])
            + dot(pick[1, span, :], below[...])
            + dot(pick[3, span, :], above[...])
        )
        far = pick[2, span, :]
        out[span, :half] = (rest[:, :half] + dot(far, far_a[...])).astype(bf16)
        out[span, half:] = (rest[:, half:] + dot(far, far_b[...])).astype(bf16)


def pick_rows(pick, own, below, far_a, far_b, above):
    return pl.pallas_call(
        pick_kernel,
        in_specs=[VM] * 6,
        out_specs=VM,
        out_shape=jax.ShapeDtypeStruct((pick.shape[1], own.shape[1]), bf16),
        compiler_params=BIG,
        name="pick",
    )(pick, own, below, far_a, far_b, above)


def mix_kernel(mix, back, own, below, far_a, far_b, above):
    tn = (((0,), (0,)), ((), ()))

    def part(m):
        return lax.dot_general(mix[m], back[...], tn, preferred_element_type=f32)

    far = part(2).astype(bf16)
    half = far_a.shape[1]
    far_a[...] = far[:, :half]
    far_b[...] = far[:, half:]
    below[...] = part(1)
    above[...] = part(3)
    own[...] = part(0)


def mix_rows(mix, back):
    rows, width = mix.shape[2], back.shape[1]
    full = jax.ShapeDtypeStruct((rows, width), f32)
    piece = jax.ShapeDtypeStruct((rows, width // 2), bf16)
    return pl.pallas_call(
        mix_kernel,
        in_specs=[VM, VM],
        out_specs=[VM] * 5,
        out_shape=[full, full, piece, piece, full],
        compiler_params=BIG,
        name="mix",
    )(mix, back)


def body(
    tokens,
    prior_state,
    mix_gain,
    in_weight,
    decay_rate,
    frequency,
    log_step,
    input_map,
    output_map,
    skip_gain,
    out_weight,
    channel_gain,
    expert_gate,
    expert_up,
    expert_down,
    shared_gate,
    shared_up,
    shared_down,
    routes,
    route_weights,
):
    experts, cores = lax.axis_size("ep"), lax.axis_size("tp")
    planes = experts // RING
    core = lax.axis_index("tp").astype(jnp.int32)
    plane = lax.axis_index("ep").astype(jnp.int32) // RING
    seq_rows, top_count = routes.shape
    slot_cap = min(seq_rows, max(2, 3 * seq_rows * top_count // (2 * experts)))
    slots = -(-4 * slot_cap // 8) * 8

    def at(z, x, t):
        return ((z % planes) * RING + x) * cores + t

    everyone = [(z, x, t) for z in range(planes) for x in range(RING) for t in range(cores)]

    def along(value, offset):
        return lax.ppermute(value, AXES, [(at(z, x, t), at(z + offset, x, t)) for z, x, t in everyone])

    def swap(value):
        return lax.ppermute(value, "tp", [(t, cores - 1 - t) for t in range(cores)])

    nearby = [
        [
            at(NEAR * (q - (t if j >= NEAR // 2 else 0)) + j, x, t)
            for j in range(NEAR)
            for x in range(RING)
        ]
        for q in range(planes // NEAR)
        for t in range(cores)
    ]

    def exchange(value):
        tiles = value.reshape(NEAR * RING, slots, value.shape[1])
        tiles = lax.all_to_all(tiles, AXES, 0, 0, axis_index_groups=nearby, tiled=True)
        return tiles.reshape(value.shape)

    table = jnp.concatenate([routes.T.astype(f32), route_weights.T], axis=0)
    tables = (table, along(table, NEAR), along(table, 2 * NEAR), along(table, -NEAR))
    base = ((plane + 2 * core) % planes) // NEAR * NEAR
    info = jnp.stack(
        [plane, core, base, jnp.int32(planes), jnp.int32(slot_cap)]
    ).astype(jnp.int32)
    pick, mix = place(info, tables, slots)

    lanes = input_map.shape[2]
    coef = turn_and_hold(decay_rate, frequency, log_step)
    imap = input_map.transpose(0, 1, 3, 2).reshape(2, -1, lanes)
    omap = output_map.reshape(2, -1, lanes)
    new_state, partial = mixer(
        tokens,
        mix_gain[None],
        in_weight,
        prior_state,
        coef,
        imap,
        omap,
        skip_gain[None],
        out_weight,
    )
    core1 = core.reshape(1)
    own, other, middle = second_norm(core1, tokens, partial, swap(partial), channel_gain[None])

    half = own.shape[1] // 2
    below, above = along(own, NEAR), along(own, -NEAR)
    far_a, far_b = along(below[:, :half], NEAR), along(above[:, half:], -NEAR)
    shared_keep, shared_send = block(
        core1, own, other, shared_gate, shared_up, shared_down, seq_rows
    )
    shared_recv = swap(shared_send)

    arrived = exchange(pick_rows(pick, own, below, far_a, far_b, above))
    keep, send = block(
        core1, arrived, swap(arrived), expert_gate[0], expert_up[0], expert_down[0], 128
    )
    summed = (keep.astype(f32) + swap(send).astype(f32)).astype(bf16)
    back = exchange(summed)

    m_own, m_below, m_far_a, m_far_b, m_above = mix_rows(mix, back)
    in_a, in_b = along(m_far_a, NEAR), along(m_far_b, -NEAR)
    to_above = jnp.concatenate(
        [m_above[:, :half] + in_a.astype(f32), m_above[:, half:]], axis=1
    ).astype(bf16)
    to_below = jnp.concatenate(
        [m_below[:, :half], m_below[:, half:] + in_b.astype(f32)], axis=1
    ).astype(bf16)
    routed = m_own + along(to_above, NEAR).astype(f32) + along(to_below, -NEAR).astype(f32)
    shared_out = shared_keep.astype(f32) + shared_recv.astype(f32)
    layer_out = (middle.astype(f32) + routed + shared_out).astype(bf16)
    return (layer_out, new_state)


def solution(mesh):
    in_specs = (
        P(("grp", "ep"), None),
        P(None, ("grp", "ep"), "tp"),
        P(),
        P(None, "tp"),
        P("tp", None),
        P("tp", None),
        P("tp"),
        P(None, "tp", None, None),
        P(None, "tp", None, None),
        P("tp"),
        P("tp", None),
        P(),
        P("ep", None, "tp"),
        P("ep", None, "tp"),
        P("ep", "tp", None),
        P(None, "tp"),
        P(None, "tp"),
        P("tp", None),
        P(("grp", "ep"), None),
        P(("grp", "ep"), None),
    )
    out_specs = (P(("grp", "ep"), "tp"), P(None, ("grp", "ep"), "tp"))
    return jax.shard_map(body, mesh=mesh, in_specs=in_specs, out_specs=out_specs, check_vma=False)
```

```python
import functools

import jax
import jax.numpy as jnp
from jax import lax
from jax.experimental import pallas as pl
from jax.experimental.pallas import tpu as pltpu
from jax.sharding import PartitionSpec as P

norm_eps = 1e-06
RING = 4
NEAR = 4
TABLE, TOP, LANES = 8, 6, 128
AXES = ("ep", "tp")
f32, bf16 = jnp.float32, jnp.bfloat16
BIG = pltpu.CompilerParams(vmem_limit_bytes=24 * 1024 * 1024)
VM = pl.BlockSpec(memory_space=pltpu.VMEM)
SM = pl.BlockSpec(memory_space=pltpu.SMEM)


def held(value):
    return pltpu.with_memory_space_constraint(value, pltpu.VMEM)


def dot(a, b):
    return jnp.dot(a, b, preferred_element_type=f32)


def scaled(values, gain):
    factor = lax.rsqrt(jnp.mean(values * values, axis=-1, keepdims=True) + norm_eps)
    return (values * factor * gain).astype(bf16)


def turn_and_hold(decay_rate, frequency, log_step):
    step_size = jnp.exp(log_step)
    real_rate = -decay_rate
    magnitude = jnp.exp(real_rate * step_size)
    turn_real = magnitude * jnp.cos(frequency * step_size)
    turn_imag = magnitude * jnp.sin(frequency * step_size)
    denominator = real_rate * real_rate + frequency * frequency
    hold_real = ((turn_real - 1.0) * real_rate + turn_imag * frequency) / denominator
    hold_imag = (turn_imag * real_rate - (turn_real - 1.0) * frequency) / denominator
    return turn_real, turn_imag, hold_real, hold_imag


def mixer_kernel(
    tok, gain, w_in, state, decay, freq, log_step, imap, omap, skip, w_out, fresh, partial, normed, acc
):
    step = pl.program_id(0)

    @pl.when(step == 0)
    def _():
        normed[...] = scaled(tok[...].astype(f32), gain[...])

    drive = dot(normed[...], w_in[...]).astype(bf16)
    chans, entries = imap.shape[1], imap.shape[2]
    groups = decay.shape[0]
    width, wide = chans // groups, groups * entries
    same = (lax.broadcasted_iota(jnp.int32, (chans, wide), 0) // width) == (
        lax.broadcasted_iota(jnp.int32, (chans, wide), 1) // entries
    )

    def spread(m):
        return jnp.where(same, jnp.concatenate([m] * groups, axis=1), 0.0).astype(bf16)

    def row(m):
        return jnp.concatenate([m[g : g + 1, :] for g in range(groups)], axis=1)

    push_re, push_im = dot(drive, spread(imap[0])), dot(drive, spread(imap[1]))
    coef = turn_and_hold(decay[...], freq[...], log_step[...])
    turn_re, turn_im, hold_re, hold_im = [row(c) for c in coef]
    old_re, old_im = state[0], state[1]
    new_re = turn_re * old_re - turn_im * old_im + (push_re * hold_re - push_im * hold_im)
    new_im = turn_re * old_im + turn_im * old_re + (push_re * hold_im + push_im * hold_re)
    fresh[0] = new_re
    fresh[1] = new_im
    nt = (((1,), (1,)), ((), ()))
    readout = lax.dot_general(
        new_re.astype(bf16), spread(omap[0]), nt, preferred_element_type=f32
    ) - lax.dot_general(new_im.astype(bf16), spread(omap[1]), nt, preferred_element_type=f32)
    readout = readout + skip[...] * drive.astype(f32)
    part = dot(jax.nn.gelu(readout).astype(bf16), w_out[...])

    @pl.when(step == 0)
    def _():
        acc[...] = part

    @pl.when(step > 0)
    def _():
        acc[...] += part

    @pl.when(step == pl.num_programs(0) - 1)
    def _():
        partial[...] = acc[...].astype(bf16)


def mixer(tokens, gain, w_in, state, decay, freq, log_step, imap, omap, skip, w_out):
    rows, width = tokens.shape
    chans = w_in.shape[1]
    groups, entries = decay.shape
    steps = 4
    c, g, s = chans // steps, groups // steps, groups * entries // steps
    return pl.pallas_call(
        mixer_kernel,
        grid=(steps,),
        in_specs=[
            VM,
            pl.BlockSpec((1, width), lambda i: (0, 0)),
            pl.BlockSpec((width, c), lambda i: (0, i)),
            pl.BlockSpec((2, rows, s), lambda i: (0, 0, i)),
            pl.BlockSpec((g, entries), lambda i: (i, 0)),
            pl.BlockSpec((g, entries), lambda i: (i, 0)),
            pl.BlockSpec((g, 1), lambda i: (i, 0)),
            pl.BlockSpec((2, c, entries), lambda i: (0, i, 0)),
            pl.BlockSpec((2, c, entries), lambda i: (0, i, 0)),
            pl.BlockSpec((1, c), lambda i: (0, i)),
            pl.BlockSpec((c, width), lambda i: (i, 0)),
        ],
        out_specs=[pl.BlockSpec((2, rows, s), lambda i: (0, 0, i)), VM],
        out_shape=[jax.ShapeDtypeStruct(state.shape, f32), pltpu.VMEM((rows, width), bf16)],
        scratch_shapes=[pltpu.VMEM((rows, width), bf16), pltpu.VMEM((rows, width), f32)],
        compiler_params=pltpu.CompilerParams(vmem_limit_bytes=56 * 1024 * 1024),
        name="mixer",
    )(tokens, gain, w_in, state, decay, freq, log_step, imap, omap, skip, w_out)


def call(kernel, scalar, arrays, outs, name, scratch=()):
    return pl.pallas_call(
        kernel,
        in_specs=[SM] + [VM] * len(arrays),
        out_specs=[VM] * len(outs),
        out_shape=[pltpu.VMEM(shape, dtype) for shape, dtype in outs],
        scratch_shapes=list(scratch),
        compiler_params=BIG,
        name=name,
    )(scalar, *[held(a) for a in arrays])


def second_norm_kernel(
    spot, tok, mine, other, gain, table, own_half, far_half, mid_half, normed, mid
):
    core = spot[0] % 2
    rows, half = far_half.shape
    middle = (tok[...].astype(f32) + (mine[...].astype(f32) + other[...].astype(f32))).astype(bf16)
    mid[...] = middle
    normed[...] = scaled(middle.astype(f32), gain[...])
    here = pl.multiple_of(core * half, half)
    there = pl.multiple_of((1 - core) * half, half)
    own_half[:rows, :] = normed[:, pl.ds(here, half)]
    own_half[rows:, :] = table[...]
    far_half[...] = normed[:, pl.ds(there, half)]
    mid_half[...] = mid[:, pl.ds(here, half)]


def second_norm(spot, tokens, mine, other, gain, table):
    rows, width = tokens.shape
    half = width // 2
    return call(
        second_norm_kernel,
        spot,
        (tokens, mine, other, gain, table),
        [((rows + TABLE, half), bf16), ((rows, half), bf16), ((rows, half), bf16)],
        "second_norm",
        [pltpu.VMEM((rows, width), bf16), pltpu.VMEM((rows, width), bf16)],
    )


def block_kernel(first, spot, own, other, gate, up, down, keep, send):
    core = spot[0] % 2
    rows, half = other.shape
    here = pl.multiple_of(core * half, half)
    there = pl.multiple_of((1 - core) * half, half)
    tile = rows // -(-rows // 256)
    for i in range(0, rows, tile):
        a, b = own[first + i : first + i + tile, :], other[i : i + tile, :]
        gate_val = dot(a, gate[pl.ds(here, half), :]) + dot(b, gate[pl.ds(there, half), :])
        up_val = dot(a, up[pl.ds(here, half), :]) + dot(b, up[pl.ds(there, half), :])
        hidden = (jax.nn.silu(gate_val) * up_val).astype(bf16)
        send[i : i + tile, :] = dot(hidden, down[:, pl.ds(there, half)]).astype(bf16)
        keep[i : i + tile, :] = dot(hidden, down[:, pl.ds(here, half)]).astype(bf16)


def block(spot, own, other, gate, up, down, first):
    return call(
        functools.partial(block_kernel, first),
        spot,
        (own, other, gate, up, down),
        [(other.shape, bf16)] * 2,
        "block",
    )


def slots_of(spot, cap, planes, slots, m, table, pick, mix):
    core, plane = spot[0] % 2, spot[0] // (2 * RING)
    base = plane + 2 * core
    base = jnp.where(base >= planes, base - planes, base) // NEAR * NEAR
    dests, rows = NEAR * RING, pick.shape[1]
    top = table.shape[0]
    order = lax.broadcasted_iota(jnp.int32, (dests, 1), 0)
    near, across = order // RING, order % RING
    at = base + near - jnp.where(near >= NEAR // 2, NEAR * core, 0)
    at = jnp.where(at < 0, at + planes, at)
    expert = (at * RING + across).astype(f32)
    before = lax.broadcasted_iota(jnp.int32, (rows, rows), 0) < lax.broadcasted_iota(
        jnp.int32, (rows, rows), 1
    )
    before = before.astype(f32).astype(bf16)
    level = lax.broadcasted_iota(jnp.int32, (slots, rows), 0).astype(f32)
    hits = jnp.zeros((dests, rows), f32)
    weight = jnp.zeros((dests, rows), f32)
    for k in range(TOP):
        hit = (table[k : k + 1, :rows] == expert).astype(f32)
        hits = hits + hit
        weight = weight + hit * table[k : k + 1, LANES : LANES + rows]
    rank = dot(hits.astype(bf16), before)
    home = plane - NEAR * m
    home = jnp.where(home < 0, home + planes, home) // NEAR
    place = jnp.where(hits > 0.5, rank + (home * cap).astype(f32), -1.0)
    for d in range(0, dests, 2):
        ones = [(level == place[e : e + 1, :]).astype(f32) for e in (d, d + 1)]
        mixed = [one * weight[e : e + 1, :] for one, e in zip(ones, (d, d + 1))]
        span = pl.ds(d * slots, 2 * slots)
        pick[span, :] = jnp.concatenate(ones, axis=0).astype(bf16)
        mix[span, :] = jnp.concatenate(mixed, axis=0).astype(bf16)


def table_of(ref, rows):
    return ref[rows:, : 2 * LANES].astype(f32)


def relay_near_kernel(cap, planes, slots, spot, own, below, above, part, mix, pick):
    rows = pick.shape[2]
    for i, (m, ref) in enumerate(((0, own), (1, below), (3, above))):
        slots_of(spot, cap, planes, slots, m, table_of(ref, rows), pick.at[i], mix.at[i])
    tile = 2 * slots
    for i in range(0, part.shape[0], tile):
        span = pl.ds(i, tile)
        total = dot(pick[0, span, :], own[:rows, :]) + dot(pick[1, span, :], below[:rows, :])
        part[span, :] = (total + dot(pick[2, span, :], above[:rows, :])).astype(bf16)


def relay_far_kernel(cap, planes, slots, spot, far_a, far_b, part, out, mix, pick):
    rows = pick.shape[1]
    half = far_a.shape[1]
    slots_of(spot, cap, planes, slots, 2, table_of(far_a, rows), pick, mix)
    tile = 2 * slots
    for i in range(0, part.shape[0], tile):
        span = pl.ds(i, tile)
        one = pick[span, :]
        out[span, :half] = part[span, :half] + dot(one, far_a[:rows, :]).astype(bf16)
        out[span, half:] = part[span, half:] + dot(one, far_b[:rows, :]).astype(bf16)


TN = (((0,), (0,)), ((), ()))


def mix_far_kernel(spot, mix, back, far_a, far_b):
    half = far_a.shape[1]
    far = lax.dot_general(mix[...], back[...], TN, preferred_element_type=f32).astype(bf16)
    far_a[...] = far[:, :half]
    far_b[...] = far[:, half:]


def mix_near_kernel(spot, mix, back, own, below, above):
    for i, ref in enumerate((own, below, above)):
        ref[...] = lax.dot_general(mix[i], back[...], TN, preferred_element_type=f32)


def join_kernel(lower, spot, sums, piece, out):
    half = piece.shape[1]
    mine, rest = (slice(0, half), slice(half, None)) if lower else (slice(half, None), slice(0, half))
    out[:, mine] = (sums[:, mine] + piece[...].astype(f32)).astype(bf16)
    out[:, rest] = sums[:, rest].astype(bf16)


def body(
    tokens,
    prior_state,
    mix_gain,
    in_weight,
    decay_rate,
    frequency,
    log_step,
    input_map,
    output_map,
    skip_gain,
    out_weight,
    channel_gain,
    expert_gate,
    expert_up,
    expert_down,
    shared_gate,
    shared_up,
    shared_down,
    routes,
    route_weights,
):
    experts, cores = lax.axis_size("ep"), lax.axis_size("tp")
    planes = experts // RING
    spot = lax.axis_index(AXES).astype(jnp.int32).reshape(1)
    seq_rows, top_count = routes.shape
    slot_cap = min(seq_rows, max(2, 3 * seq_rows * top_count // (2 * experts)))
    slots = -(-4 * slot_cap // 8) * 8
    total = NEAR * RING * slots
    width = tokens.shape[1]
    wide = width // 2
    half = wide // 2

    def at(z, x, t):
        return ((z % planes) * RING + x) * cores + t

    everyone = [(z, x, t) for z in range(planes) for x in range(RING) for t in range(cores)]

    def along(value, offset):
        return lax.ppermute(value, AXES, [(at(z, x, t), at(z + offset, x, t)) for z, x, t in everyone])

    def swap(value):
        return lax.ppermute(value, "tp", [(t, cores - 1 - t) for t in range(cores)])

    nearby = [
        [
            at(NEAR * (q - (t if j >= NEAR // 2 else 0)) + j, x, t)
            for j in range(NEAR)
            for x in range(RING)
        ]
        for q in range(planes // NEAR)
        for t in range(cores)
    ]

    def exchange(value):
        tiles = value.reshape(NEAR * RING, slots, value.shape[1])
        tiles = lax.all_to_all(tiles, AXES, 0, 0, axis_index_groups=nearby, tiled=True)
        return tiles.reshape(value.shape)

    table = jnp.concatenate(
        [
            jnp.pad(value.T.astype(bf16), ((0, TABLE - top_count), (0, LANES - seq_rows)))
            for value in (routes, route_weights)
        ],
        axis=1,
    )
    table = jnp.pad(table, ((0, 0), (0, wide - 2 * LANES)))

    lanes = input_map.shape[2]
    imap = input_map.transpose(0, 1, 3, 2).reshape(2, -1, lanes)
    omap = output_map.reshape(2, -1, lanes)
    new_state, partial = mixer(
        tokens,
        mix_gain[None],
        in_weight,
        prior_state,
        decay_rate,
        frequency,
        log_step[:, None],
        imap,
        omap,
        skip_gain[None],
        out_weight,
    )
    own, other, middle = second_norm(
        spot, tokens, partial, swap(partial), channel_gain[None], table
    )

    below, above = along(own, NEAR), along(own, -NEAR)
    far_a, far_b = along(below[:, :half], NEAR), along(above[:seq_rows, half:], -NEAR)
    shared_keep, shared_send = block(
        spot, own[:seq_rows], other, shared_gate, shared_up, shared_down, 0
    )
    shared_recv = swap(shared_send)
    sizes = (slot_cap, planes, slots)
    part, mix_near = call(
        functools.partial(relay_near_kernel, *sizes),
        spot,
        (own, below, above),
        [((total, wide), bf16), ((3, total, seq_rows), bf16)],
        "relay_near",
        [pltpu.VMEM((3, total, seq_rows), bf16)],
    )
    part, shared_keep, shared_recv = lax.optimization_barrier((part, shared_keep, shared_recv))
    rows, mix_far = call(
        functools.partial(relay_far_kernel, *sizes),
        spot,
        (far_a, far_b, part),
        [((total, wide), bf16), ((total, seq_rows), bf16)],
        "relay_far",
        [pltpu.VMEM((total, seq_rows), bf16)],
    )

    arrived = exchange(rows)
    cut = total // 2
    others = [swap(arrived[i : i + cut]) for i in (0, cut)]
    weights = (expert_gate[0], expert_up[0], expert_down[0])
    outs = [block(spot, arrived, o, *weights, i) for o, i in zip(others, (0, cut))]
    summed = [keep.astype(f32) + swap(send).astype(f32) for keep, send in outs]
    back = exchange(jnp.concatenate(summed, axis=0).astype(bf16))

    piece = ((seq_rows, half), bf16)
    sums = ((seq_rows, wide), f32)
    m_far_a, m_far_b = call(mix_far_kernel, spot, (mix_far, back), [piece] * 2, "mix_far")
    in_a, in_b = along(m_far_a, NEAR), along(m_far_b, -NEAR)
    m_own, m_below, m_above = call(
        mix_near_kernel, spot, (mix_near, back), [sums] * 3, "mix_near"
    )

    def join(lower, value, arriving):
        return call(
            functools.partial(join_kernel, lower),
            spot,
            (value, arriving),
            [((seq_rows, wide), bf16)],
            "join",
        )[0]

    from_below = along(join(True, m_above, in_a), NEAR)
    from_above = along(join(False, m_below, in_b), -NEAR)
    routed = m_own + from_below.astype(f32) + from_above.astype(f32)
    shared_out = shared_keep.astype(f32) + shared_recv.astype(f32)
    layer_out = (middle.astype(f32) + routed + shared_out).astype(bf16)
    return (layer_out, new_state)


def solution(mesh):
    in_specs = (
        P(("grp", "ep"), None),
        P(None, ("grp", "ep"), "tp"),
        P(),
        P(None, "tp"),
        P("tp", None),
        P("tp", None),
        P("tp"),
        P(None, "tp", None, None),
        P(None, "tp", None, None),
        P("tp"),
        P("tp", None),
        P(),
        P("ep", None, "tp"),
        P("ep", None, "tp"),
        P("ep", "tp", None),
        P(None, "tp"),
        P(None, "tp"),
        P("tp", None),
        P(("grp", "ep"), None),
        P(("grp", "ep"), None),
    )
    out_specs = (P(("grp", "ep"), "tp"), P(None, ("grp", "ep"), "tp"))
    return jax.shard_map(body, mesh=mesh, in_specs=in_specs, out_specs=out_specs, check_vma=False)
```

```python
import functools

import jax
import jax.numpy as jnp
from jax import lax
from jax.experimental import pallas as pl
from jax.experimental.pallas import tpu as pltpu
from jax.sharding import PartitionSpec as P

norm_eps = 1e-06
RING = 4
NEAR = 4
TABLE, TOP, LANES = 8, 6, 128
AXES = ("ep", "tp")
f32, bf16 = jnp.float32, jnp.bfloat16
BIG = pltpu.CompilerParams(vmem_limit_bytes=24 * 1024 * 1024)
VM = pl.BlockSpec(memory_space=pltpu.VMEM)
SM = pl.BlockSpec(memory_space=pltpu.SMEM)


def held(value):
    return pltpu.with_memory_space_constraint(value, pltpu.VMEM)


def dot(a, b):
    return jnp.dot(a, b, preferred_element_type=f32)


def scaled(values, gain):
    factor = lax.rsqrt(jnp.mean(values * values, axis=-1, keepdims=True) + norm_eps)
    return (values * factor * gain).astype(bf16)


def turn_and_hold(decay_rate, frequency, log_step):
    step_size = jnp.exp(log_step)
    real_rate = -decay_rate
    magnitude = jnp.exp(real_rate * step_size)
    turn_real = magnitude * jnp.cos(frequency * step_size)
    turn_imag = magnitude * jnp.sin(frequency * step_size)
    denominator = real_rate * real_rate + frequency * frequency
    hold_real = ((turn_real - 1.0) * real_rate + turn_imag * frequency) / denominator
    hold_imag = (turn_imag * real_rate - (turn_real - 1.0) * frequency) / denominator
    return turn_real, turn_imag, hold_real, hold_imag


def mixer_kernel(
    tok, gain, w_in, state, decay, freq, log_step, imap, omap, skip, w_out, fresh, partial, normed, acc
):
    step = pl.program_id(0)

    @pl.when(step == 0)
    def _():
        normed[...] = scaled(tok[...].astype(f32), gain[...])

    drive = dot(normed[...], w_in[...]).astype(bf16)
    chans, entries = imap.shape[1], imap.shape[2]
    groups = decay.shape[0]
    width, wide = chans // groups, groups * entries
    same = (lax.broadcasted_iota(jnp.int32, (chans, wide), 0) // width) == (
        lax.broadcasted_iota(jnp.int32, (chans, wide), 1) // entries
    )

    def spread(m):
        return jnp.where(same, jnp.concatenate([m] * groups, axis=1), 0.0).astype(bf16)

    def row(m):
        return jnp.concatenate([m[g : g + 1, :] for g in range(groups)], axis=1)

    push_re, push_im = dot(drive, spread(imap[0])), dot(drive, spread(imap[1]))
    spread_out = (groups, log_step.shape[1])
    wanted = step * groups + lax.broadcasted_iota(jnp.int32, spread_out, 0)
    chosen = wanted == lax.broadcasted_iota(jnp.int32, spread_out, 1)
    log_steps = jnp.sum(jnp.where(chosen, log_step[...], 0.0), axis=1, keepdims=True)
    coef = turn_and_hold(decay[...], freq[...], log_steps)
    turn_re, turn_im, hold_re, hold_im = [row(c) for c in coef]
    old_re, old_im = state[0], state[1]
    new_re = turn_re * old_re - turn_im * old_im + (push_re * hold_re - push_im * hold_im)
    new_im = turn_re * old_im + turn_im * old_re + (push_re * hold_im + push_im * hold_re)
    fresh[0] = new_re
    fresh[1] = new_im
    nt = (((1,), (1,)), ((), ()))
    readout = lax.dot_general(
        new_re.astype(bf16), spread(omap[0]), nt, preferred_element_type=f32
    ) - lax.dot_general(new_im.astype(bf16), spread(omap[1]), nt, preferred_element_type=f32)
    readout = readout + skip[...] * drive.astype(f32)
    part = dot(jax.nn.gelu(readout).astype(bf16), w_out[...])

    @pl.when(step == 0)
    def _():
        acc[...] = part

    @pl.when(step > 0)
    def _():
        acc[...] += part

    @pl.when(step == pl.num_programs(0) - 1)
    def _():
        partial[...] = acc[...].astype(bf16)


def mixer(tokens, gain, w_in, state, decay, freq, log_step, imap, omap, skip, w_out):
    rows, width = tokens.shape
    chans = w_in.shape[1]
    groups, entries = decay.shape
    steps = 4
    c, g, s = chans // steps, groups // steps, groups * entries // steps
    return pl.pallas_call(
        mixer_kernel,
        grid=(steps,),
        in_specs=[
            VM,
            pl.BlockSpec((1, width), lambda i: (0, 0)),
            pl.BlockSpec((width, c), lambda i: (0, i)),
            pl.BlockSpec((2, rows, s), lambda i: (0, 0, i)),
            pl.BlockSpec((g, entries), lambda i: (i, 0)),
            pl.BlockSpec((g, entries), lambda i: (i, 0)),
            pl.BlockSpec((1, groups), lambda i: (0, 0)),
            pl.BlockSpec((2, c, entries), lambda i: (0, i, 0)),
            pl.BlockSpec((2, c, entries), lambda i: (0, i, 0)),
            pl.BlockSpec((1, c), lambda i: (0, i)),
            pl.BlockSpec((c, width), lambda i: (i, 0)),
        ],
        out_specs=[pl.BlockSpec((2, rows, s), lambda i: (0, 0, i)), VM],
        out_shape=[jax.ShapeDtypeStruct(state.shape, f32), pltpu.VMEM((rows, width), bf16)],
        scratch_shapes=[pltpu.VMEM((rows, width), bf16), pltpu.VMEM((rows, width), f32)],
        compiler_params=pltpu.CompilerParams(vmem_limit_bytes=56 * 1024 * 1024),
        name="mixer",
    )(tokens, gain, w_in, state, decay, freq, log_step, imap, omap, skip, w_out)


def call(kernel, scalar, arrays, outs, scratch=()):
    return pl.pallas_call(
        kernel,
        in_specs=[SM] + [VM] * len(arrays),
        out_specs=[VM] * len(outs),
        out_shape=[pltpu.VMEM(shape, dtype) for shape, dtype in outs],
        scratch_shapes=list(scratch),
        compiler_params=BIG,
    )(scalar, *[held(a) for a in arrays])


def second_norm_kernel(
    spot, tok, mine, other, gain, table, own_half, far_half, mid_half, left, right, normed, mid
):
    core = spot[0] % 2
    rows, half = far_half.shape
    middle = (tok[...].astype(f32) + (mine[...].astype(f32) + other[...].astype(f32))).astype(bf16)
    mid[...] = middle
    normed[...] = scaled(middle.astype(f32), gain[...])
    here = pl.multiple_of(core * half, half)
    there = pl.multiple_of((1 - core) * half, half)
    own = normed[:, pl.ds(here, half)]
    own_half[...] = own
    left[:rows, :] = own[:, : half // 2]
    left[rows:, :] = table[...]
    right[...] = own[:, half // 2 :]
    far_half[...] = normed[:, pl.ds(there, half)]
    mid_half[...] = mid[:, pl.ds(here, half)]


def second_norm(spot, tokens, mine, other, gain, table):
    rows, width = tokens.shape
    half = width // 2
    return call(
        second_norm_kernel,
        spot,
        (tokens, mine, other, gain, table),
        [((rows, half), bf16)] * 3
        + [((rows + TABLE, half // 2), bf16), ((rows, half // 2), bf16)],
        [pltpu.VMEM((rows, width), bf16), pltpu.VMEM((rows, width), bf16)],
    )


def block_kernel(first, spot, own, other, gate, up, down, keep, send):
    core = spot[0] % 2
    rows, half = other.shape
    here = pl.multiple_of(core * half, half)
    there = pl.multiple_of((1 - core) * half, half)
    tile = rows // -(-rows // 256)
    for i in range(0, rows, tile):
        a, b = own[first + i : first + i + tile, :], other[i : i + tile, :]
        gate_val = dot(a, gate[pl.ds(here, half), :]) + dot(b, gate[pl.ds(there, half), :])
        up_val = dot(a, up[pl.ds(here, half), :]) + dot(b, up[pl.ds(there, half), :])
        hidden = (jax.nn.silu(gate_val) * up_val).astype(bf16)
        send[i : i + tile, :] = dot(hidden, down[:, pl.ds(there, half)]).astype(bf16)
        keep[i : i + tile, :] = dot(hidden, down[:, pl.ds(here, half)]).astype(bf16)


def block(spot, own, other, gate, up, down, first):
    return call(
        functools.partial(block_kernel, first),
        spot,
        (own, other, gate, up, down),
        [(other.shape, bf16)] * 2,
    )


def slots_of(spot, cap, planes, slots, m, table, pick, mix):
    core, plane = spot[0] % 2, spot[0] // (2 * RING)
    base = plane + 2 * core
    base = jnp.where(base >= planes, base - planes, base) // NEAR * NEAR
    dests, rows = NEAR * RING, pick.shape[1]
    order = lax.broadcasted_iota(jnp.int32, (dests, 1), 0)
    near, across = order // RING, order % RING
    at = base + near - jnp.where(near >= NEAR // 2, NEAR * core, 0)
    at = jnp.where(at < 0, at + planes, at)
    expert = (at * RING + across).astype(f32)
    before = lax.broadcasted_iota(jnp.int32, (rows, rows), 0) < lax.broadcasted_iota(
        jnp.int32, (rows, rows), 1
    )
    before = before.astype(f32).astype(bf16)
    level = lax.broadcasted_iota(jnp.int32, (slots, rows), 0).astype(f32)
    hits = jnp.zeros((dests, rows), f32)
    weight = jnp.zeros((dests, rows), f32)
    for k in range(TOP):
        hit = (table[k : k + 1, :rows] == expert).astype(f32)
        hits = hits + hit
        weight = weight + hit * table[k : k + 1, LANES : LANES + rows]
    rank = dot(hits.astype(bf16), before)
    home = plane - NEAR * m
    home = jnp.where(home < 0, home + planes, home) // NEAR
    place = jnp.where(hits > 0.5, rank + (home * cap).astype(f32), -1.0)
    for d in range(0, dests, 2):
        ones = [(level == place[e : e + 1, :]).astype(f32) for e in (d, d + 1)]
        mixed = [one * weight[e : e + 1, :] for one, e in zip(ones, (d, d + 1))]
        span = pl.ds(d * slots, 2 * slots)
        pick[span, :] = jnp.concatenate(ones, axis=0).astype(bf16)
        mix[span, :] = jnp.concatenate(mixed, axis=0).astype(bf16)


def table_of(ref, rows):
    return ref[rows:, : 2 * LANES].astype(f32)


def relay_near_kernel(
    cap, planes, slots, spot, own_l, own_r, below_l, below_r, above_l, above_r, part, mix, pick
):
    rows = pick.shape[2]
    half = own_r.shape[1]
    for i, (m, ref) in enumerate(((0, own_l), (1, below_l), (3, above_l))):
        slots_of(spot, cap, planes, slots, m, table_of(ref, rows), pick.at[i], mix.at[i])
    tile = 2 * slots
    for i in range(0, part.shape[0], tile):
        span = pl.ds(i, tile)
        for at, refs in (
            (slice(0, half), (own_l, below_l, above_l)),
            (slice(half, None), (own_r, below_r, above_r)),
        ):
            sums = [dot(pick[n, span, :], ref[:rows, :]) for n, ref in enumerate(refs)]
            part[span, at] = (sums[0] + sums[1] + sums[2]).astype(bf16)


def relay_far_kernel(cap, planes, slots, spot, far_l, far_r, part, out, mix, pick):
    rows = pick.shape[1]
    half = far_r.shape[1]
    slots_of(spot, cap, planes, slots, 2, table_of(far_l, rows), pick, mix)
    tile = 2 * slots
    for i in range(0, part.shape[0], tile):
        span = pl.ds(i, tile)
        one = pick[span, :]
        out[span, :half] = part[span, :half] + dot(one, far_l[:rows, :]).astype(bf16)
        out[span, half:] = part[span, half:] + dot(one, far_r[...]).astype(bf16)


TN = (((0,), (0,)), ((), ()))


def mix_far_kernel(spot, mix, back, left, right):
    half = left.shape[1]
    far = lax.dot_general(mix[...], back[...], TN, preferred_element_type=f32).astype(bf16)
    left[...] = far[:, :half]
    right[...] = far[:, half:]


def mix_near_kernel(spot, mix, back, own, below_l, below_r, above_l, above_r):
    half = below_l.shape[1]
    for i, (left, right) in ((1, (below_l, below_r)), (2, (above_l, above_r))):
        sums = lax.dot_general(mix[i], back[...], TN, preferred_element_type=f32)
        left[...] = sums[:, :half].astype(left.dtype)
        right[...] = sums[:, half:].astype(right.dtype)
    own[...] = lax.dot_general(mix[0], back[...], TN, preferred_element_type=f32)


def body(
    tokens,
    prior_state,
    mix_gain,
    in_weight,
    decay_rate,
    frequency,
    log_step,
    input_map,
    output_map,
    skip_gain,
    out_weight,
    channel_gain,
    expert_gate,
    expert_up,
    expert_down,
    shared_gate,
    shared_up,
    shared_down,
    routes,
    route_weights,
):
    experts, cores = lax.axis_size("ep"), lax.axis_size("tp")
    planes = experts // RING
    spot = lax.axis_index(AXES).astype(jnp.int32).reshape(1)
    seq_rows, top_count = routes.shape
    slot_cap = min(seq_rows, max(2, 3 * seq_rows * top_count // (2 * experts)))
    slots = -(-4 * slot_cap // 8) * 8
    total = NEAR * RING * slots
    width = tokens.shape[1]
    wide = width // 2
    half = wide // 2

    def at(z, x, t):
        return ((z % planes) * RING + x) * cores + t

    everyone = [(z, x, t) for z in range(planes) for x in range(RING) for t in range(cores)]

    def along(value, offset):
        return lax.ppermute(
            value, AXES, [(at(z, x, t), at(z + offset, x, t)) for z, x, t in everyone]
        )

    def swap(value):
        return lax.ppermute(value, "tp", [(t, cores - 1 - t) for t in range(cores)])

    nearby = [
        [
            at(NEAR * (q - (t if j >= NEAR // 2 else 0)) + j, x, t)
            for j in range(NEAR)
            for x in range(RING)
        ]
        for q in range(planes // NEAR)
        for t in range(cores)
    ]

    def exchange(value):
        tiles = value.reshape(NEAR * RING, slots, value.shape[1])
        tiles = lax.all_to_all(tiles, AXES, 0, 0, axis_index_groups=nearby, tiled=True)
        return tiles.reshape(value.shape)

    table = jnp.concatenate(
        [
            jnp.pad(value.T.astype(bf16), ((0, TABLE - top_count), (0, LANES - seq_rows)))
            for value in (routes, route_weights)
        ],
        axis=1,
    )
    table = jnp.pad(table, ((0, 0), (0, half - 2 * LANES)))

    lanes = input_map.shape[2]
    imap = input_map.transpose(0, 1, 3, 2).reshape(2, -1, lanes)
    omap = output_map.reshape(2, -1, lanes)
    new_state, partial = mixer(
        tokens,
        mix_gain[None],
        in_weight,
        prior_state,
        decay_rate,
        frequency,
        log_step[None],
        imap,
        omap,
        skip_gain[None],
        out_weight,
    )
    own, other, middle, own_l, own_r = second_norm(
        spot, tokens, partial, swap(partial), channel_gain[None], table
    )

    below_l, above_r = along(own_l, NEAR), along(own_r, -NEAR)
    below_r, above_l = along(own_r, NEAR), along(own_l, -NEAR)
    far_l, far_r = along(below_l, NEAR), along(above_r, -NEAR)
    shared_keep, shared_send = block(spot, own, other, shared_gate, shared_up, shared_down, 0)
    shared_recv = swap(shared_send)
    sizes = (slot_cap, planes, slots)
    part, mix_near = call(
        functools.partial(relay_near_kernel, *sizes),
        spot,
        (own_l, own_r, below_l, below_r, above_l, above_r),
        [((total, wide), bf16), ((3, total, seq_rows), bf16)],
        [pltpu.VMEM((3, total, seq_rows), bf16)],
    )
    part, shared_keep, shared_recv = lax.optimization_barrier((part, shared_keep, shared_recv))
    rows, mix_far = call(
        functools.partial(relay_far_kernel, *sizes),
        spot,
        (far_l, far_r, part),
        [((total, wide), bf16), ((total, seq_rows), bf16)],
        [pltpu.VMEM((total, seq_rows), bf16)],
    )

    arrived = exchange(rows)
    cut = total // 2
    others = [swap(arrived[i : i + cut]) for i in (0, cut)]
    weights = (expert_gate[0], expert_up[0], expert_down[0])
    outs = [block(spot, arrived, o, *weights, i) for o, i in zip(others, (0, cut))]
    summed = [keep.astype(f32) + swap(send).astype(f32) for keep, send in outs]
    back = exchange(jnp.concatenate(summed, axis=0).astype(bf16))

    sent, sums = ((seq_rows, half), bf16), ((seq_rows, half), f32)
    m_far_l, m_far_r = call(mix_far_kernel, spot, (mix_far, back), [sent] * 2)
    in_l, in_r = along(m_far_l, NEAR), along(m_far_r, -NEAR)
    m_own, m_below_l, m_below_r, m_above_l, m_above_r = call(
        mix_near_kernel, spot, (mix_near, back), [((seq_rows, wide), f32), sent, sums, sums, sent]
    )
    below_right, above_left = along(m_above_r, NEAR), along(m_below_l, -NEAR)
    below_left = along((m_above_l + in_l.astype(f32)).astype(bf16), NEAR)
    above_right = along((m_below_r + in_r.astype(f32)).astype(bf16), -NEAR)
    shared_out = shared_keep.astype(f32) + shared_recv.astype(f32)
    rest = middle.astype(f32) + shared_out + m_own
    left = rest[:, :half] + below_left.astype(f32) + above_left.astype(f32)
    right = rest[:, half:] + below_right.astype(f32) + above_right.astype(f32)
    layer_out = jnp.concatenate([left, right], axis=1).astype(bf16)
    return (layer_out, new_state)


def solution(mesh):
    in_specs = (
        P(("grp", "ep"), None),
        P(None, ("grp", "ep"), "tp"),
        P(),
        P(None, "tp"),
        P("tp", None),
        P("tp", None),
        P("tp"),
        P(None, "tp", None, None),
        P(None, "tp", None, None),
        P("tp"),
        P("tp", None),
        P(),
        P("ep", None, "tp"),
        P("ep", None, "tp"),
        P("ep", "tp", None),
        P(None, "tp"),
        P(None, "tp"),
        P("tp", None),
        P(("grp", "ep"), None),
        P(("grp", "ep"), None),
    )
    out_specs = (P(("grp", "ep"), "tp"), P(None, ("grp", "ep"), "tp"))
    return jax.shard_map(body, mesh=mesh, in_specs=in_specs, out_specs=out_specs, check_vma=False)
```

```python
import functools

import jax
import jax.numpy as jnp
from jax import lax
from jax.experimental import pallas as pl
from jax.experimental.pallas import tpu as pltpu
from jax.sharding import PartitionSpec as P

norm_eps = 1e-06
RING = 4
NEAR = 4
TABLE, TOP, LANES = 8, 6, 128
AXES = ("ep", "tp")
f32, bf16 = jnp.float32, jnp.bfloat16
BIG = pltpu.CompilerParams(vmem_limit_bytes=24 * 1024 * 1024)
VM = pl.BlockSpec(memory_space=pltpu.VMEM)
SM = pl.BlockSpec(memory_space=pltpu.SMEM)


def held(value):
    return pltpu.with_memory_space_constraint(value, pltpu.VMEM)


def dot(a, b):
    return jnp.dot(a, b, preferred_element_type=f32)


def scaled(values, gain):
    factor = lax.rsqrt(jnp.mean(values * values, axis=-1, keepdims=True) + norm_eps)
    return (values * factor * gain).astype(bf16)


def turn_and_hold(decay_rate, frequency, log_step):
    step_size = jnp.exp(log_step)
    real_rate = -decay_rate
    magnitude = jnp.exp(real_rate * step_size)
    turn_real = magnitude * jnp.cos(frequency * step_size)
    turn_imag = magnitude * jnp.sin(frequency * step_size)
    denominator = real_rate * real_rate + frequency * frequency
    hold_real = ((turn_real - 1.0) * real_rate + turn_imag * frequency) / denominator
    hold_imag = (turn_imag * real_rate - (turn_real - 1.0) * frequency) / denominator
    return turn_real, turn_imag, hold_real, hold_imag


def mixer_kernel(
    tok, gain, w_in, state, decay, freq, log_step, imap, omap, skip, w_out, fresh, partial, normed, acc
):
    step = pl.program_id(0)

    @pl.when(step == 0)
    def _():
        normed[...] = scaled(tok[...].astype(f32), gain[...])

    drive = dot(normed[...], w_in[...]).astype(bf16)
    chans, entries = imap.shape[1], imap.shape[2]
    groups = decay.shape[0]
    width, wide = chans // groups, groups * entries
    same = (lax.broadcasted_iota(jnp.int32, (chans, wide), 0) // width) == (
        lax.broadcasted_iota(jnp.int32, (chans, wide), 1) // entries
    )

    def spread(m):
        return jnp.where(same, jnp.concatenate([m] * groups, axis=1), 0.0).astype(bf16)

    def row(m):
        return jnp.concatenate([m[g : g + 1, :] for g in range(groups)], axis=1)

    push_re, push_im = dot(drive, spread(imap[0])), dot(drive, spread(imap[1]))
    spread_out = (groups, log_step.shape[1])
    wanted = step * groups + lax.broadcasted_iota(jnp.int32, spread_out, 0)
    chosen = wanted == lax.broadcasted_iota(jnp.int32, spread_out, 1)
    log_steps = jnp.sum(jnp.where(chosen, log_step[...], 0.0), axis=1, keepdims=True)
    coef = turn_and_hold(decay[...], freq[...], log_steps)
    turn_re, turn_im, hold_re, hold_im = [row(c) for c in coef]
    old_re, old_im = state[0], state[1]
    new_re = turn_re * old_re - turn_im * old_im + (push_re * hold_re - push_im * hold_im)
    new_im = turn_re * old_im + turn_im * old_re + (push_re * hold_im + push_im * hold_re)
    fresh[0] = new_re
    fresh[1] = new_im
    nt = (((1,), (1,)), ((), ()))
    readout = lax.dot_general(
        new_re.astype(bf16), spread(omap[0]), nt, preferred_element_type=f32
    ) - lax.dot_general(new_im.astype(bf16), spread(omap[1]), nt, preferred_element_type=f32)
    readout = readout + skip[...] * drive.astype(f32)
    part = dot(jax.nn.gelu(readout).astype(bf16), w_out[...])

    @pl.when(step == 0)
    def _():
        acc[...] = part

    @pl.when(step > 0)
    def _():
        acc[...] += part

    @pl.when(step == pl.num_programs(0) - 1)
    def _():
        partial[...] = acc[...].astype(bf16)


def mixer(tokens, gain, w_in, state, decay, freq, log_step, imap, omap, skip, w_out):
    rows, width = tokens.shape
    chans = w_in.shape[1]
    groups, entries = decay.shape
    steps = 4
    c, g, s = chans // steps, groups // steps, groups * entries // steps
    return pl.pallas_call(
        mixer_kernel,
        grid=(steps,),
        in_specs=[
            VM,
            pl.BlockSpec((1, width), lambda i: (0, 0)),
            pl.BlockSpec((width, c), lambda i: (0, i)),
            pl.BlockSpec((2, rows, s), lambda i: (0, 0, i)),
            pl.BlockSpec((g, entries), lambda i: (i, 0)),
            pl.BlockSpec((g, entries), lambda i: (i, 0)),
            pl.BlockSpec((1, groups), lambda i: (0, 0)),
            pl.BlockSpec((2, c, entries), lambda i: (0, i, 0)),
            pl.BlockSpec((2, c, entries), lambda i: (0, i, 0)),
            pl.BlockSpec((1, c), lambda i: (0, i)),
            pl.BlockSpec((c, width), lambda i: (i, 0)),
        ],
        out_specs=[pl.BlockSpec((2, rows, s), lambda i: (0, 0, i)), VM],
        out_shape=[jax.ShapeDtypeStruct(state.shape, f32), pltpu.VMEM((rows, width), bf16)],
        scratch_shapes=[pltpu.VMEM((rows, width), bf16), pltpu.VMEM((rows, width), f32)],
        compiler_params=pltpu.CompilerParams(vmem_limit_bytes=56 * 1024 * 1024),
        name="mixer",
    )(tokens, gain, w_in, state, decay, freq, log_step, imap, omap, skip, w_out)


def call(kernel, scalar, arrays, outs, scratch=()):
    return pl.pallas_call(
        kernel,
        in_specs=[SM] + [VM] * len(arrays),
        out_specs=[VM] * len(outs),
        out_shape=[pltpu.VMEM(shape, dtype) for shape, dtype in outs],
        scratch_shapes=list(scratch),
        compiler_params=BIG,
    )(scalar, *[held(a) for a in arrays])


def second_norm_kernel(
    spot, tok, mine, other, gain, table, own_half, far_half, mid_half, left, right, normed, mid
):
    core = spot[0] % 2
    rows, half = far_half.shape
    middle = (tok[...].astype(f32) + (mine[...].astype(f32) + other[...].astype(f32))).astype(bf16)
    mid[...] = middle
    normed[...] = scaled(middle.astype(f32), gain[...])
    here = pl.multiple_of(core * half, half)
    there = pl.multiple_of((1 - core) * half, half)
    own = normed[:, pl.ds(here, half)]
    own_half[...] = own
    left[:rows, :] = own[:, : half // 2]
    left[rows:, :] = table[...]
    right[...] = own[:, half // 2 :]
    far_half[...] = normed[:, pl.ds(there, half)]
    mid_half[...] = mid[:, pl.ds(here, half)]


def second_norm(spot, tokens, mine, other, gain, table):
    rows, width = tokens.shape
    half = width // 2
    return call(
        second_norm_kernel,
        spot,
        (tokens, mine, other, gain, table),
        [((rows, half), bf16)] * 3
        + [((rows + TABLE, half // 2), bf16), ((rows, half // 2), bf16)],
        [pltpu.VMEM((rows, width), bf16), pltpu.VMEM((rows, width), bf16)],
    )


def block_kernel(first, spot, own, other, gate, up, down, keep, send):
    core = spot[0] % 2
    rows, half = other.shape
    here = pl.multiple_of(core * half, half)
    there = pl.multiple_of((1 - core) * half, half)
    tile = rows // -(-rows // 256)
    for i in range(0, rows, tile):
        a, b = own[first + i : first + i + tile, :], other[i : i + tile, :]
        gate_val = dot(a, gate[pl.ds(here, half), :]) + dot(b, gate[pl.ds(there, half), :])
        up_val = dot(a, up[pl.ds(here, half), :]) + dot(b, up[pl.ds(there, half), :])
        hidden = (jax.nn.silu(gate_val) * up_val).astype(bf16)
        send[i : i + tile, :] = dot(hidden, down[:, pl.ds(there, half)]).astype(bf16)
        keep[i : i + tile, :] = dot(hidden, down[:, pl.ds(here, half)]).astype(bf16)


def block(spot, own, other, gate, up, down, first):
    return call(
        functools.partial(block_kernel, first),
        spot,
        (own, other, gate, up, down),
        [(other.shape, bf16)] * 2,
    )


def slots_of(spot, cap, planes, slots, m, table, pick, mix):
    core, plane = spot[0] % 2, spot[0] // (2 * RING)
    base = plane + 2 * core
    base = jnp.where(base >= planes, base - planes, base) // NEAR * NEAR
    dests, rows = NEAR * RING, pick.shape[1]
    order = lax.broadcasted_iota(jnp.int32, (dests, 1), 0)
    near, across = order // RING, order % RING
    at = base + near - jnp.where(near >= NEAR // 2, NEAR * core, 0)
    at = jnp.where(at < 0, at + planes, at)
    expert = (at * RING + across).astype(f32)
    before = lax.broadcasted_iota(jnp.int32, (rows, rows), 0) < lax.broadcasted_iota(
        jnp.int32, (rows, rows), 1
    )
    before = before.astype(f32).astype(bf16)
    level = lax.broadcasted_iota(jnp.int32, (slots, rows), 0).astype(f32)
    hits = jnp.zeros((dests, rows), f32)
    weight = jnp.zeros((dests, rows), f32)
    for k in range(TOP):
        hit = (table[k : k + 1, :rows] == expert).astype(f32)
        hits = hits + hit
        weight = weight + hit * table[k : k + 1, LANES : LANES + rows]
    rank = dot(hits.astype(bf16), before)
    home = plane // NEAR
    clusters = planes // NEAR
    home = (home, home + 1 - 2 * (home % 2), (home + clusters // 2) % clusters, clusters - 1 - home)[m]
    place = jnp.where(hits > 0.5, rank + (home * cap).astype(f32), -1.0)
    for d in range(0, dests, 2):
        ones = [(level == place[e : e + 1, :]).astype(f32) for e in (d, d + 1)]
        mixed = [one * weight[e : e + 1, :] for one, e in zip(ones, (d, d + 1))]
        span = pl.ds(d * slots, 2 * slots)
        pick[span, :] = jnp.concatenate(ones, axis=0).astype(bf16)
        mix[span, :] = jnp.concatenate(mixed, axis=0).astype(bf16)


def table_of(ref, rows):
    return ref[rows:, : 2 * LANES].astype(f32)


def relay_near_kernel(
    cap, planes, slots, spot, own_l, own_r, below_l, below_r, above_l, above_r, part, mix, pick
):
    rows = pick.shape[2]
    half = own_r.shape[1]
    for i, (m, ref) in enumerate(((0, own_l), (1, below_l), (3, above_l))):
        slots_of(spot, cap, planes, slots, m, table_of(ref, rows), pick.at[i], mix.at[i])
    tile = 2 * slots
    for i in range(0, part.shape[0], tile):
        span = pl.ds(i, tile)
        for at, refs in (
            (slice(0, half), (own_l, below_l, above_l)),
            (slice(half, None), (own_r, below_r, above_r)),
        ):
            sums = [dot(pick[n, span, :], ref[:rows, :]) for n, ref in enumerate(refs)]
            part[span, at] = (sums[0] + sums[1] + sums[2]).astype(bf16)


def relay_far_kernel(cap, planes, slots, spot, far_l, far_r, part, out, mix, pick):
    rows = pick.shape[1]
    half = far_r.shape[1]
    slots_of(spot, cap, planes, slots, 2, table_of(far_l, rows), pick, mix)
    tile = 2 * slots
    for i in range(0, part.shape[0], tile):
        span = pl.ds(i, tile)
        one = pick[span, :]
        out[span, :half] = part[span, :half] + dot(one, far_l[:rows, :]).astype(bf16)
        out[span, half:] = part[span, half:] + dot(one, far_r[...]).astype(bf16)


TN = (((0,), (0,)), ((), ()))


def mix_far_kernel(spot, mix, back, left, right):
    half = left.shape[1]
    far = lax.dot_general(mix[...], back[...], TN, preferred_element_type=f32).astype(bf16)
    left[...] = far[:, :half]
    right[...] = far[:, half:]


def mix_near_kernel(spot, mix, back, own, below_l, below_r, above_l, above_r):
    half = below_l.shape[1]
    for i, (left, right) in ((1, (below_l, below_r)), (2, (above_l, above_r))):
        sums = lax.dot_general(mix[i], back[...], TN, preferred_element_type=f32)
        left[...] = sums[:, :half].astype(left.dtype)
        right[...] = sums[:, half:].astype(right.dtype)
    own[...] = lax.dot_general(mix[0], back[...], TN, preferred_element_type=f32)


def body(
    tokens,
    prior_state,
    mix_gain,
    in_weight,
    decay_rate,
    frequency,
    log_step,
    input_map,
    output_map,
    skip_gain,
    out_weight,
    channel_gain,
    expert_gate,
    expert_up,
    expert_down,
    shared_gate,
    shared_up,
    shared_down,
    routes,
    route_weights,
):
    experts, cores = lax.axis_size("ep"), lax.axis_size("tp")
    planes = experts // RING
    spot = lax.axis_index(AXES).astype(jnp.int32).reshape(1)
    seq_rows, top_count = routes.shape
    slot_cap = min(seq_rows, max(2, 3 * seq_rows * top_count // (2 * experts)))
    slots = -(-4 * slot_cap // 8) * 8
    total = NEAR * RING * slots
    width = tokens.shape[1]
    wide = width // 2
    half = wide // 2

    def at(z, x, t):
        return ((z % planes) * RING + x) * cores + t

    everyone = [(z, x, t) for z in range(planes) for x in range(RING) for t in range(cores)]

    def pair(value, shift):
        def mate(z):
            up = (z // NEAR + shift) % 2 == 0
            return z + NEAR if up else z - NEAR

        return lax.ppermute(value, AXES, [(at(z, x, t), at(mate(z), x, t)) for z, x, t in everyone])

    def swap(value):
        return lax.ppermute(value, "tp", [(t, cores - 1 - t) for t in range(cores)])

    nearby = [
        [
            at(NEAR * (q - (t if j >= NEAR // 2 else 0)) + j, x, t)
            for j in range(NEAR)
            for x in range(RING)
        ]
        for q in range(planes // NEAR)
        for t in range(cores)
    ]

    def exchange(value):
        tiles = value.reshape(NEAR * RING, slots, value.shape[1])
        tiles = lax.all_to_all(tiles, AXES, 0, 0, axis_index_groups=nearby, tiled=True)
        return tiles.reshape(value.shape)

    table = jnp.concatenate(
        [
            jnp.pad(value.T.astype(bf16), ((0, TABLE - top_count), (0, LANES - seq_rows)))
            for value in (routes, route_weights)
        ],
        axis=1,
    )
    table = jnp.pad(table, ((0, 0), (0, half - 2 * LANES)))

    lanes = input_map.shape[2]
    imap = input_map.transpose(0, 1, 3, 2).reshape(2, -1, lanes)
    omap = output_map.reshape(2, -1, lanes)
    new_state, partial = mixer(
        tokens,
        mix_gain[None],
        in_weight,
        prior_state,
        decay_rate,
        frequency,
        log_step[None],
        imap,
        omap,
        skip_gain[None],
        out_weight,
    )
    own, other, middle, own_l, own_r = second_norm(
        spot, tokens, partial, swap(partial), channel_gain[None], table
    )

    below_l, above_r = pair(own_l, 0), pair(own_r, 1)
    below_r, above_l = pair(own_r, 0), pair(own_l, 1)
    far_l, far_r = pair(below_l, 1), pair(above_r, 0)
    shared_keep, shared_send = block(spot, own, other, shared_gate, shared_up, shared_down, 0)
    shared_recv = swap(shared_send)
    sizes = (slot_cap, planes, slots)
    part, mix_near = call(
        functools.partial(relay_near_kernel, *sizes),
        spot,
        (own_l, own_r, below_l, below_r, above_l, above_r),
        [((total, wide), bf16), ((3, total, seq_rows), bf16)],
        [pltpu.VMEM((3, total, seq_rows), bf16)],
    )
    part, shared_keep, shared_recv = lax.optimization_barrier((part, shared_keep, shared_recv))
    rows, mix_far = call(
        functools.partial(relay_far_kernel, *sizes),
        spot,
        (far_l, far_r, part),
        [((total, wide), bf16), ((total, seq_rows), bf16)],
        [pltpu.VMEM((total, seq_rows), bf16)],
    )

    arrived = exchange(rows)
    cut = total // 2
    others = [swap(arrived[i : i + cut]) for i in (0, cut)]
    weights = (expert_gate[0], expert_up[0], expert_down[0])
    outs = [block(spot, arrived, o, *weights, i) for o, i in zip(others, (0, cut))]
    summed = [keep.astype(f32) + swap(send).astype(f32) for keep, send in outs]
    back = exchange(jnp.concatenate(summed, axis=0).astype(bf16))

    sent, sums = ((seq_rows, half), bf16), ((seq_rows, half), f32)
    m_far_l, m_far_r = call(mix_far_kernel, spot, (mix_far, back), [sent] * 2)
    in_l, in_r = pair(m_far_l, 0), pair(m_far_r, 1)
    m_own, m_below_l, m_below_r, m_above_l, m_above_r = call(
        mix_near_kernel, spot, (mix_near, back), [((seq_rows, wide), f32), sent, sums, sums, sent]
    )
    above_right, below_left = pair(m_above_r, 1), pair(m_below_l, 0)
    above_left = pair((m_above_l + in_l.astype(f32)).astype(bf16), 1)
    below_right = pair((m_below_r + in_r.astype(f32)).astype(bf16), 0)
    shared_out = shared_keep.astype(f32) + shared_recv.astype(f32)
    rest = middle.astype(f32) + shared_out + m_own
    left = rest[:, :half] + below_left.astype(f32) + above_left.astype(f32)
    right = rest[:, half:] + below_right.astype(f32) + above_right.astype(f32)
    layer_out = jnp.concatenate([left, right], axis=1).astype(bf16)
    return (layer_out, new_state)


def solution(mesh):
    in_specs = (
        P(("grp", "ep"), None),
        P(None, ("grp", "ep"), "tp"),
        P(),
        P(None, "tp"),
        P("tp", None),
        P("tp", None),
        P("tp"),
        P(None, "tp", None, None),
        P(None, "tp", None, None),
        P("tp"),
        P("tp", None),
        P(),
        P("ep", None, "tp"),
        P("ep", None, "tp"),
        P("ep", "tp", None),
        P(None, "tp"),
        P(None, "tp"),
        P("tp", None),
        P(("grp", "ep"), None),
        P(("grp", "ep"), None),
    )
    out_specs = (P(("grp", "ep"), "tp"), P(None, ("grp", "ep"), "tp"))
    return jax.shard_map(body, mesh=mesh, in_specs=in_specs, out_specs=out_specs, check_vma=False)
```

```python
import functools

import jax
import jax.numpy as jnp
from jax import lax
from jax.experimental import pallas as pl
from jax.experimental.pallas import tpu as pltpu
from jax.sharding import PartitionSpec as P

norm_eps = 1e-06
RING = 4
NEAR = 4
TABLE, TOP, LANES = 8, 6, 128
AXES = ("ep", "tp")
f32, bf16 = jnp.float32, jnp.bfloat16
BIG = pltpu.CompilerParams(vmem_limit_bytes=24 * 1024 * 1024)
VM = pl.BlockSpec(memory_space=pltpu.VMEM)
SM = pl.BlockSpec(memory_space=pltpu.SMEM)


def held(value):
    return pltpu.with_memory_space_constraint(value, pltpu.VMEM)


def dot(a, b):
    return jnp.dot(a, b, preferred_element_type=f32)


def scaled(values, gain):
    factor = lax.rsqrt(jnp.mean(values * values, axis=-1, keepdims=True) + norm_eps)
    return (values * factor * gain).astype(bf16)


def turn_and_hold(decay_rate, frequency, log_step):
    step_size = jnp.exp(log_step)
    real_rate = -decay_rate
    magnitude = jnp.exp(real_rate * step_size)
    turn_real = magnitude * jnp.cos(frequency * step_size)
    turn_imag = magnitude * jnp.sin(frequency * step_size)
    denominator = real_rate * real_rate + frequency * frequency
    hold_real = ((turn_real - 1.0) * real_rate + turn_imag * frequency) / denominator
    hold_imag = (turn_imag * real_rate - (turn_real - 1.0) * frequency) / denominator
    return turn_real, turn_imag, hold_real, hold_imag


def mixer_kernel(
    tok, gain, w_in, state, decay, freq, log_step, imap, omap, skip, w_out, fresh, partial, normed, acc
):
    step = pl.program_id(0)

    @pl.when(step == 0)
    def _():
        normed[...] = scaled(tok[...].astype(f32), gain[...])

    drive = dot(normed[...], w_in[...]).astype(bf16)
    chans, entries = imap.shape[1], imap.shape[2]
    groups = decay.shape[0]
    width, wide = chans // groups, groups * entries
    same = (lax.broadcasted_iota(jnp.int32, (chans, wide), 0) // width) == (
        lax.broadcasted_iota(jnp.int32, (chans, wide), 1) // entries
    )

    def spread(m):
        return jnp.where(same, jnp.concatenate([m] * groups, axis=1), 0.0).astype(bf16)

    def row(m):
        return jnp.concatenate([m[g : g + 1, :] for g in range(groups)], axis=1)

    push_re, push_im = dot(drive, spread(imap[0])), dot(drive, spread(imap[1]))
    spread_out = (groups, log_step.shape[1])
    wanted = step * groups + lax.broadcasted_iota(jnp.int32, spread_out, 0)
    chosen = wanted == lax.broadcasted_iota(jnp.int32, spread_out, 1)
    log_steps = jnp.sum(jnp.where(chosen, log_step[...], 0.0), axis=1, keepdims=True)
    coef = turn_and_hold(decay[...], freq[...], log_steps)
    turn_re, turn_im, hold_re, hold_im = [row(c) for c in coef]
    old_re, old_im = state[0], state[1]
    new_re = turn_re * old_re - turn_im * old_im + (push_re * hold_re - push_im * hold_im)
    new_im = turn_re * old_im + turn_im * old_re + (push_re * hold_im + push_im * hold_re)
    fresh[0] = new_re
    fresh[1] = new_im
    nt = (((1,), (1,)), ((), ()))
    readout = lax.dot_general(
        new_re.astype(bf16), spread(omap[0]), nt, preferred_element_type=f32
    ) - lax.dot_general(new_im.astype(bf16), spread(omap[1]), nt, preferred_element_type=f32)
    readout = readout + skip[...] * drive.astype(f32)
    part = dot(jax.nn.gelu(readout).astype(bf16), w_out[...])

    @pl.when(step == 0)
    def _():
        acc[...] = part

    @pl.when(step > 0)
    def _():
        acc[...] += part

    @pl.when(step == pl.num_programs(0) - 1)
    def _():
        partial[...] = acc[...].astype(bf16)


def mixer(tokens, gain, w_in, state, decay, freq, log_step, imap, omap, skip, w_out):
    rows, width = tokens.shape
    chans = w_in.shape[1]
    groups, entries = decay.shape
    steps = 2
    c, g, s = chans // steps, groups // steps, groups * entries // steps
    return pl.pallas_call(
        mixer_kernel,
        grid=(steps,),
        in_specs=[
            VM,
            pl.BlockSpec((1, width), lambda i: (0, 0)),
            pl.BlockSpec((width, c), lambda i: (0, i)),
            pl.BlockSpec((2, rows, s), lambda i: (0, 0, i)),
            pl.BlockSpec((g, entries), lambda i: (i, 0)),
            pl.BlockSpec((g, entries), lambda i: (i, 0)),
            pl.BlockSpec((1, groups), lambda i: (0, 0)),
            pl.BlockSpec((2, c, entries), lambda i: (0, i, 0)),
            pl.BlockSpec((2, c, entries), lambda i: (0, i, 0)),
            pl.BlockSpec((1, c), lambda i: (0, i)),
            pl.BlockSpec((c, width), lambda i: (i, 0)),
        ],
        out_specs=[pl.BlockSpec((2, rows, s), lambda i: (0, 0, i)), VM],
        out_shape=[jax.ShapeDtypeStruct(state.shape, f32), pltpu.VMEM((rows, width), bf16)],
        scratch_shapes=[pltpu.VMEM((rows, width), bf16), pltpu.VMEM((rows, width), f32)],
        compiler_params=pltpu.CompilerParams(vmem_limit_bytes=56 * 1024 * 1024),
        name="mixer",
    )(tokens, gain, w_in, state, decay, freq, log_step, imap, omap, skip, w_out)


def call(kernel, scalar, arrays, outs, scratch=()):
    return pl.pallas_call(
        kernel,
        in_specs=[SM] + [VM] * len(arrays),
        out_specs=[VM] * len(outs),
        out_shape=[pltpu.VMEM(shape, dtype) for shape, dtype in outs],
        scratch_shapes=list(scratch),
        compiler_params=BIG,
    )(scalar, *[held(a) for a in arrays])


def second_norm_kernel(
    spot, tok, mine, other, gain, table, own_half, far_half, mid_half, left, right, normed, mid
):
    core = spot[0] % 2
    rows, half = far_half.shape
    middle = (tok[...].astype(f32) + (mine[...].astype(f32) + other[...].astype(f32))).astype(bf16)
    mid[...] = middle
    normed[...] = scaled(middle.astype(f32), gain[...])
    here = pl.multiple_of(core * half, half)
    there = pl.multiple_of((1 - core) * half, half)
    own = normed[:, pl.ds(here, half)]
    own_half[...] = own
    left[:rows, :] = own[:, : half // 2]
    left[rows:, :] = table[...]
    right[...] = own[:, half // 2 :]
    far_half[...] = normed[:, pl.ds(there, half)]
    mid_half[...] = mid[:, pl.ds(here, half)]


def second_norm(spot, tokens, mine, other, gain, table):
    rows, width = tokens.shape
    half = width // 2
    return call(
        second_norm_kernel,
        spot,
        (tokens, mine, other, gain, table),
        [((rows, half), bf16)] * 3
        + [((rows + TABLE, half // 2), bf16), ((rows, half // 2), bf16)],
        [pltpu.VMEM((rows, width), bf16), pltpu.VMEM((rows, width), bf16)],
    )


def halves(spot, half):
    core = spot[0] % 2
    here = pl.multiple_of(core * half, half)
    there = pl.multiple_of((1 - core) * half, half)
    return pl.ds(here, half), pl.ds(there, half)


def tiles(rows):
    size = rows // -(-rows // 256)
    return [slice(i, i + size) for i in range(0, rows, size)]


def entry_kernel(spot, own, gate, up, part):
    here, _ = halves(spot, own.shape[1])
    hidden = gate.shape[1]
    for rows in tiles(own.shape[0]):
        part[rows, :hidden] = dot(own[rows, :], gate[here, :])
        part[rows, hidden:] = dot(own[rows, :], up[here, :])


def rest_kernel(first, spot, part, other, gate, up, down, keep, send):
    here, there = halves(spot, other.shape[1])
    hidden = gate.shape[1]
    for rows in tiles(other.shape[0]):
        done = slice(first + rows.start, first + rows.stop)
        gate_val = part[done, :hidden] + dot(other[rows, :], gate[there, :])
        up_val = part[done, hidden:] + dot(other[rows, :], up[there, :])
        value = (jax.nn.silu(gate_val) * up_val).astype(bf16)
        send[rows, :] = dot(value, down[:, there]).astype(bf16)
        keep[rows, :] = dot(value, down[:, here]).astype(bf16)


def entry(spot, own, gate, up):
    shape = (own.shape[0], gate.shape[1] + up.shape[1])
    return call(entry_kernel, spot, (own, gate, up), [(shape, f32)])[0]


def rest(spot, part, other, gate, up, down, first):
    return call(
        functools.partial(rest_kernel, first),
        spot,
        (part, other, gate, up, down),
        [(other.shape, bf16)] * 2,
    )


def slots_of(spot, cap, planes, slots, m, table, pick, mix):
    core, plane = spot[0] % 2, spot[0] // (2 * RING)
    base = plane + 2 * core
    base = jnp.where(base >= planes, base - planes, base) // NEAR * NEAR
    dests, rows = NEAR * RING, pick.shape[1]
    order = lax.broadcasted_iota(jnp.int32, (dests, 1), 0)
    near, across = order // RING, order % RING
    at = base + near - jnp.where(near >= NEAR // 2, NEAR * core, 0)
    at = jnp.where(at < 0, at + planes, at)
    expert = (at * RING + across).astype(f32)
    before = lax.broadcasted_iota(jnp.int32, (rows, rows), 0) < lax.broadcasted_iota(
        jnp.int32, (rows, rows), 1
    )
    before = before.astype(f32).astype(bf16)
    level = lax.broadcasted_iota(jnp.int32, (slots, rows), 0).astype(f32)
    hits = jnp.zeros((dests, rows), f32)
    weight = jnp.zeros((dests, rows), f32)
    for k in range(TOP):
        hit = (table[k : k + 1, :rows] == expert).astype(f32)
        hits = hits + hit
        weight = weight + hit * table[k : k + 1, LANES : LANES + rows]
    rank = dot(hits.astype(bf16), before)
    home = plane // NEAR
    clusters = planes // NEAR
    home = (home, home + 1 - 2 * (home % 2), (home + clusters // 2) % clusters, clusters - 1 - home)[m]
    place = jnp.where(hits > 0.5, rank + (home * cap).astype(f32), -1.0)
    for d in range(0, dests, 2):
        ones = [(level == place[e : e + 1, :]).astype(f32) for e in (d, d + 1)]
        mixed = [one * weight[e : e + 1, :] for one, e in zip(ones, (d, d + 1))]
        span = pl.ds(d * slots, 2 * slots)
        pick[span, :] = jnp.concatenate(ones, axis=0).astype(bf16)
        mix[span, :] = jnp.concatenate(mixed, axis=0).astype(bf16)


def table_of(ref, rows):
    return ref[rows:, : 2 * LANES].astype(f32)


def relay_near_kernel(
    cap, planes, slots, spot, own_l, own_r, below_l, below_r, above_l, above_r, part, mix, pick
):
    rows = pick.shape[2]
    half = own_r.shape[1]
    for i, (m, ref) in enumerate(((0, own_l), (1, below_l), (3, above_l))):
        slots_of(spot, cap, planes, slots, m, table_of(ref, rows), pick.at[i], mix.at[i])
    tile = 2 * slots
    for i in range(0, part.shape[0], tile):
        span = pl.ds(i, tile)
        for at, refs in (
            (slice(0, half), (own_l, below_l, above_l)),
            (slice(half, None), (own_r, below_r, above_r)),
        ):
            sums = [dot(pick[n, span, :], ref[:rows, :]) for n, ref in enumerate(refs)]
            part[span, at] = (sums[0] + sums[1] + sums[2]).astype(bf16)


def relay_far_kernel(cap, planes, slots, spot, far_l, far_r, part, out, mix, pick):
    rows = pick.shape[1]
    half = far_r.shape[1]
    slots_of(spot, cap, planes, slots, 2, table_of(far_l, rows), pick, mix)
    tile = 2 * slots
    for i in range(0, part.shape[0], tile):
        span = pl.ds(i, tile)
        one = pick[span, :]
        out[span, :half] = part[span, :half] + dot(one, far_l[:rows, :]).astype(bf16)
        out[span, half:] = part[span, half:] + dot(one, far_r[...]).astype(bf16)


TN = (((0,), (0,)), ((), ()))


def mix_far_kernel(spot, mix, back, left, right):
    half = left.shape[1]
    far = lax.dot_general(mix[...], back[...], TN, preferred_element_type=f32).astype(bf16)
    left[...] = far[:, :half]
    right[...] = far[:, half:]


def mix_near_kernel(spot, mix, back, own, below_l, below_r, above_l, above_r):
    half = below_l.shape[1]
    for i, (left, right) in ((1, (below_l, below_r)), (2, (above_l, above_r))):
        sums = lax.dot_general(mix[i], back[...], TN, preferred_element_type=f32)
        left[...] = sums[:, :half].astype(left.dtype)
        right[...] = sums[:, half:].astype(right.dtype)
    own[...] = lax.dot_general(mix[0], back[...], TN, preferred_element_type=f32)


def body(
    tokens,
    prior_state,
    mix_gain,
    in_weight,
    decay_rate,
    frequency,
    log_step,
    input_map,
    output_map,
    skip_gain,
    out_weight,
    channel_gain,
    expert_gate,
    expert_up,
    expert_down,
    shared_gate,
    shared_up,
    shared_down,
    routes,
    route_weights,
):
    experts, cores = lax.axis_size("ep"), lax.axis_size("tp")
    planes = experts // RING
    spot = lax.axis_index(AXES).astype(jnp.int32).reshape(1)
    seq_rows, top_count = routes.shape
    slot_cap = min(seq_rows, max(2, 3 * seq_rows * top_count // (2 * experts)))
    slots = -(-4 * slot_cap // 8) * 8
    total = NEAR * RING * slots
    width = tokens.shape[1]
    wide = width // 2
    half = wide // 2

    def at(z, x, t):
        return ((z % planes) * RING + x) * cores + t

    everyone = [(z, x, t) for z in range(planes) for x in range(RING) for t in range(cores)]

    def pair(value, shift):
        def mate(z):
            up = (z // NEAR + shift) % 2 == 0
            return z + NEAR if up else z - NEAR

        return lax.ppermute(value, AXES, [(at(z, x, t), at(mate(z), x, t)) for z, x, t in everyone])

    def swap(value):
        return lax.ppermute(value, "tp", [(t, cores - 1 - t) for t in range(cores)])

    nearby = [
        [
            at(NEAR * (q - (t if j >= NEAR // 2 else 0)) + j, x, t)
            for j in range(NEAR)
            for x in range(RING)
        ]
        for q in range(planes // NEAR)
        for t in range(cores)
    ]

    def exchange(value):
        tiles = value.reshape(NEAR * RING, slots, value.shape[1])
        tiles = lax.all_to_all(tiles, AXES, 0, 0, axis_index_groups=nearby, tiled=True)
        return tiles.reshape(value.shape)

    table = jnp.concatenate(
        [
            jnp.pad(value.T.astype(bf16), ((0, TABLE - top_count), (0, LANES - seq_rows)))
            for value in (routes, route_weights)
        ],
        axis=1,
    )
    table = jnp.pad(table, ((0, 0), (0, half - 2 * LANES)))

    lanes = input_map.shape[2]
    imap = input_map.transpose(0, 1, 3, 2).reshape(2, -1, lanes)
    omap = output_map.reshape(2, -1, lanes)
    new_state, partial = mixer(
        tokens,
        mix_gain[None],
        in_weight,
        prior_state,
        decay_rate,
        frequency,
        log_step[None],
        imap,
        omap,
        skip_gain[None],
        out_weight,
    )
    own, other, middle, own_l, own_r = second_norm(
        spot, tokens, partial, swap(partial), channel_gain[None], table
    )

    below_l, above_r = pair(own_l, 0), pair(own_r, 1)
    below_r, above_l = pair(own_r, 0), pair(own_l, 1)
    far_l, far_r = pair(below_l, 1), pair(above_r, 0)
    shared_part = entry(spot, own, shared_gate, shared_up)
    shared_keep, shared_send = rest(
        spot, shared_part, other, shared_gate, shared_up, shared_down, 0
    )
    shared_recv = swap(shared_send)
    sizes = (slot_cap, planes, slots)
    part, mix_near = call(
        functools.partial(relay_near_kernel, *sizes),
        spot,
        (own_l, own_r, below_l, below_r, above_l, above_r),
        [((total, wide), bf16), ((3, total, seq_rows), bf16)],
        [pltpu.VMEM((3, total, seq_rows), bf16)],
    )
    part, shared_keep, shared_recv = lax.optimization_barrier((part, shared_keep, shared_recv))
    rows, mix_far = call(
        functools.partial(relay_far_kernel, *sizes),
        spot,
        (far_l, far_r, part),
        [((total, wide), bf16), ((total, seq_rows), bf16)],
        [pltpu.VMEM((total, seq_rows), bf16)],
    )

    arrived = exchange(rows)
    cut = total * 4 // 7
    weights = (expert_gate[0], expert_up[0], expert_down[0])
    others = [swap(arrived[:cut]), swap(arrived[cut:])]
    part = entry(spot, arrived, *weights[:2])
    outs = []
    for other, first in zip(others, (0, cut)):
        outs.append(rest(spot, part, other, *weights, first))
    summed = [keep.astype(f32) + swap(send).astype(f32) for keep, send in outs]
    back = exchange(jnp.concatenate(summed, axis=0).astype(bf16))

    sent, sums = ((seq_rows, half), bf16), ((seq_rows, half), f32)
    m_far_l, m_far_r = call(mix_far_kernel, spot, (mix_far, back), [sent] * 2)
    in_l, in_r = pair(m_far_l, 0), pair(m_far_r, 1)
    m_own, m_below_l, m_below_r, m_above_l, m_above_r = call(
        mix_near_kernel, spot, (mix_near, back), [((seq_rows, wide), f32), sent, sums, sums, sent]
    )
    above_right, below_left = pair(m_above_r, 1), pair(m_below_l, 0)
    above_left = pair((m_above_l + in_l.astype(f32)).astype(bf16), 1)
    below_right = pair((m_below_r + in_r.astype(f32)).astype(bf16), 0)
    shared_out = shared_keep.astype(f32) + shared_recv.astype(f32)
    known = middle.astype(f32) + shared_out + m_own
    left = known[:, :half] + below_left.astype(f32) + above_left.astype(f32)
    right = known[:, half:] + below_right.astype(f32) + above_right.astype(f32)
    layer_out = jnp.concatenate([left, right], axis=1).astype(bf16)
    return (layer_out, new_state)


def solution(mesh):
    in_specs = (
        P(("grp", "ep"), None),
        P(None, ("grp", "ep"), "tp"),
        P(),
        P(None, "tp"),
        P("tp", None),
        P("tp", None),
        P("tp"),
        P(None, "tp", None, None),
        P(None, "tp", None, None),
        P("tp"),
        P("tp", None),
        P(),
        P("ep", None, "tp"),
        P("ep", None, "tp"),
        P("ep", "tp", None),
        P(None, "tp"),
        P(None, "tp"),
        P("tp", None),
        P(("grp", "ep"), None),
        P(("grp", "ep"), None),
    )
    out_specs = (P(("grp", "ep"), "tp"), P(None, ("grp", "ep"), "tp"))
    return jax.shard_map(body, mesh=mesh, in_specs=in_specs, out_specs=out_specs, check_vma=False)
```

```python
import functools

import jax
import jax.numpy as jnp
from jax import lax
from jax.experimental import pallas as pl
from jax.experimental.pallas import tpu as pltpu
from jax.sharding import PartitionSpec as P

norm_eps = 1e-06
RING = 4
NEAR = 4
TABLE, TOP, LANES = 8, 6, 128
AXES = ("ep", "tp")
f32, bf16 = jnp.float32, jnp.bfloat16
BIG = pltpu.CompilerParams(vmem_limit_bytes=24 * 1024 * 1024)
VM = pl.BlockSpec(memory_space=pltpu.VMEM)
SM = pl.BlockSpec(memory_space=pltpu.SMEM)


def held(value):
    return pltpu.with_memory_space_constraint(value, pltpu.VMEM)


def dot(a, b):
    return jnp.dot(a, b, preferred_element_type=f32)


def scaled(values, gain):
    factor = lax.rsqrt(jnp.mean(values * values, axis=-1, keepdims=True) + norm_eps)
    return (values * factor * gain).astype(bf16)


def turn_and_hold(decay_rate, frequency, log_step):
    step_size = jnp.exp(log_step)
    real_rate = -decay_rate
    magnitude = jnp.exp(real_rate * step_size)
    turn_real = magnitude * jnp.cos(frequency * step_size)
    turn_imag = magnitude * jnp.sin(frequency * step_size)
    denominator = real_rate * real_rate + frequency * frequency
    hold_real = ((turn_real - 1.0) * real_rate + turn_imag * frequency) / denominator
    hold_imag = (turn_imag * real_rate - (turn_real - 1.0) * frequency) / denominator
    return turn_real, turn_imag, hold_real, hold_imag


def mixer_kernel(
    tok, gain, w_in, state, decay, freq, log_step, imap, omap, skip, w_out, fresh, partial, normed, acc
):
    step = pl.program_id(0)

    @pl.when(step == 0)
    def _():
        normed[...] = scaled(tok[...].astype(f32), gain[...])

    drive = dot(normed[...], w_in[...]).astype(bf16)
    chans, entries = imap.shape[1], imap.shape[2]
    groups = decay.shape[0]
    width, wide = chans // groups, groups * entries
    same = (lax.broadcasted_iota(jnp.int32, (chans, wide), 0) // width) == (
        lax.broadcasted_iota(jnp.int32, (chans, wide), 1) // entries
    )

    def spread(m):
        return jnp.where(same, jnp.concatenate([m] * groups, axis=1), 0.0).astype(bf16)

    def row(m):
        return jnp.concatenate([m[g : g + 1, :] for g in range(groups)], axis=1)

    push_re, push_im = dot(drive, spread(imap[0])), dot(drive, spread(imap[1]))
    spread_out = (groups, log_step.shape[1])
    wanted = step * groups + lax.broadcasted_iota(jnp.int32, spread_out, 0)
    chosen = wanted == lax.broadcasted_iota(jnp.int32, spread_out, 1)
    log_steps = jnp.sum(jnp.where(chosen, log_step[...], 0.0), axis=1, keepdims=True)
    coef = turn_and_hold(decay[...], freq[...], log_steps)
    turn_re, turn_im, hold_re, hold_im = [row(c) for c in coef]
    old_re, old_im = state[0], state[1]
    new_re = turn_re * old_re - turn_im * old_im + (push_re * hold_re - push_im * hold_im)
    new_im = turn_re * old_im + turn_im * old_re + (push_re * hold_im + push_im * hold_re)
    fresh[0] = new_re
    fresh[1] = new_im
    nt = (((1,), (1,)), ((), ()))
    readout = lax.dot_general(
        new_re.astype(bf16), spread(omap[0]), nt, preferred_element_type=f32
    ) - lax.dot_general(new_im.astype(bf16), spread(omap[1]), nt, preferred_element_type=f32)
    readout = readout + skip[...] * drive.astype(f32)
    part = dot(jax.nn.gelu(readout).astype(bf16), w_out[...])

    @pl.when(step == 0)
    def _():
        acc[...] = part

    @pl.when(step > 0)
    def _():
        acc[...] += part

    @pl.when(step == pl.num_programs(0) - 1)
    def _():
        partial[...] = acc[...].astype(bf16)


def mixer(tokens, gain, w_in, state, decay, freq, log_step, imap, omap, skip, w_out):
    rows, width = tokens.shape
    chans = w_in.shape[1]
    groups, entries = decay.shape
    steps = 2
    c, g, s = chans // steps, groups // steps, groups * entries // steps
    return pl.pallas_call(
        mixer_kernel,
        grid=(steps,),
        in_specs=[
            VM,
            pl.BlockSpec((1, width), lambda i: (0, 0)),
            pl.BlockSpec((width, c), lambda i: (0, i)),
            pl.BlockSpec((2, rows, s), lambda i: (0, 0, i)),
            pl.BlockSpec((g, entries), lambda i: (i, 0)),
            pl.BlockSpec((g, entries), lambda i: (i, 0)),
            pl.BlockSpec((1, groups), lambda i: (0, 0)),
            pl.BlockSpec((2, c, entries), lambda i: (0, i, 0)),
            pl.BlockSpec((2, c, entries), lambda i: (0, i, 0)),
            pl.BlockSpec((1, c), lambda i: (0, i)),
            pl.BlockSpec((c, width), lambda i: (i, 0)),
        ],
        out_specs=[pl.BlockSpec((2, rows, s), lambda i: (0, 0, i)), VM],
        out_shape=[jax.ShapeDtypeStruct(state.shape, f32), pltpu.VMEM((rows, width), bf16)],
        scratch_shapes=[pltpu.VMEM((rows, width), bf16), pltpu.VMEM((rows, width), f32)],
        compiler_params=pltpu.CompilerParams(vmem_limit_bytes=56 * 1024 * 1024),
        name="mixer",
    )(tokens, gain, w_in, state, decay, freq, log_step, imap, omap, skip, w_out)


def call(kernel, scalar, arrays, outs, scratch=()):
    return pl.pallas_call(
        kernel,
        in_specs=[SM] + [VM] * len(arrays),
        out_specs=[VM] * len(outs),
        out_shape=[pltpu.VMEM(shape, dtype) for shape, dtype in outs],
        scratch_shapes=list(scratch),
        compiler_params=BIG,
    )(scalar, *[held(a) for a in arrays])


def second_norm_kernel(
    spot, tok, mine, other, gain, table, own_half, far_half, mid_half, travel, normed, mid
):
    core = spot[0] % 2
    rows, half = far_half.shape
    middle = (tok[...].astype(f32) + (mine[...].astype(f32) + other[...].astype(f32))).astype(bf16)
    mid[...] = middle
    normed[...] = scaled(middle.astype(f32), gain[...])
    here = pl.multiple_of(core * half, half)
    there = pl.multiple_of((1 - core) * half, half)
    own = normed[:, pl.ds(here, half)]
    own_half[...] = own
    travel[:rows, :] = own
    travel[rows:, :] = table[...]
    far_half[...] = normed[:, pl.ds(there, half)]
    mid_half[...] = mid[:, pl.ds(here, half)]


def second_norm(spot, tokens, mine, other, gain, table):
    rows, width = tokens.shape
    half = width // 2
    return call(
        second_norm_kernel,
        spot,
        (tokens, mine, other, gain, table),
        [((rows, half), bf16)] * 3
        + [((rows + TABLE, half), bf16)],
        [pltpu.VMEM((rows, width), bf16), pltpu.VMEM((rows, width), bf16)],
    )


def halves(spot, half):
    core = spot[0] % 2
    here = pl.multiple_of(core * half, half)
    there = pl.multiple_of((1 - core) * half, half)
    return pl.ds(here, half), pl.ds(there, half)


def tiles(rows):
    size = rows // -(-rows // 256)
    return [slice(i, i + size) for i in range(0, rows, size)]


def entry_kernel(spot, own, gate, up, part):
    here, _ = halves(spot, own.shape[1])
    hidden = gate.shape[1]
    for rows in tiles(own.shape[0]):
        part[rows, :hidden] = dot(own[rows, :], gate[here, :])
        part[rows, hidden:] = dot(own[rows, :], up[here, :])


def rest_kernel(first, spot, part, other, gate, up, down, keep, send):
    here, there = halves(spot, other.shape[1])
    hidden = gate.shape[1]
    for rows in tiles(other.shape[0]):
        done = slice(first + rows.start, first + rows.stop)
        gate_val = part[done, :hidden] + dot(other[rows, :], gate[there, :])
        up_val = part[done, hidden:] + dot(other[rows, :], up[there, :])
        value = (jax.nn.silu(gate_val) * up_val).astype(bf16)
        send[rows, :] = dot(value, down[:, there]).astype(bf16)
        keep[rows, :] = dot(value, down[:, here]).astype(bf16)


def entry(spot, own, gate, up):
    shape = (own.shape[0], gate.shape[1] + up.shape[1])
    return call(entry_kernel, spot, (own, gate, up), [(shape, f32)])[0]


def rest(spot, part, other, gate, up, down, first):
    return call(
        functools.partial(rest_kernel, first),
        spot,
        (part, other, gate, up, down),
        [(other.shape, bf16)] * 2,
    )


def slots_of(spot, cap, planes, slots, m, table, pick, mix):
    core, plane = spot[0] % 2, spot[0] // (2 * RING)
    base = plane + 2 * core
    base = jnp.where(base >= planes, base - planes, base) // NEAR * NEAR
    dests, rows = NEAR * RING, pick.shape[1]
    order = lax.broadcasted_iota(jnp.int32, (dests, 1), 0)
    near, across = order // RING, order % RING
    at = base + near - jnp.where(near >= NEAR // 2, NEAR * core, 0)
    at = jnp.where(at < 0, at + planes, at)
    expert = (at * RING + across).astype(f32)
    before = lax.broadcasted_iota(jnp.int32, (rows, rows), 0) < lax.broadcasted_iota(
        jnp.int32, (rows, rows), 1
    )
    before = before.astype(f32).astype(bf16)
    level = lax.broadcasted_iota(jnp.int32, (slots, rows), 0).astype(f32)
    hits = jnp.zeros((dests, rows), f32)
    weight = jnp.zeros((dests, rows), f32)
    for k in range(TOP):
        hit = (table[k : k + 1, :rows] == expert).astype(f32)
        hits = hits + hit
        weight = weight + hit * table[k : k + 1, LANES : LANES + rows]
    rank = dot(hits.astype(bf16), before)
    home = plane // NEAR
    clusters = planes // NEAR
    even, odd = home + 1 - 2 * (home % 2), clusters - 1 - home
    first, second = jnp.where(core == 0, even, odd), jnp.where(core == 0, odd, even)
    home = (home, first, (home + clusters // 2) % clusters, second)[m]
    place = jnp.where(hits > 0.5, rank + (home * cap).astype(f32), -1.0)
    for d in range(0, dests, 2):
        ones = [(level == place[e : e + 1, :]).astype(f32) for e in (d, d + 1)]
        mixed = [one * weight[e : e + 1, :] for one, e in zip(ones, (d, d + 1))]
        span = pl.ds(d * slots, 2 * slots)
        pick[span, :] = jnp.concatenate(ones, axis=0).astype(bf16)
        mix[span, :] = jnp.concatenate(mixed, axis=0).astype(bf16)


def table_of(ref, rows):
    return ref[rows:, : 2 * LANES].astype(f32)


def relay_near_kernel(cap, planes, slots, spot, own, below, above, part, mix, pick):
    rows = pick.shape[2]
    sources = (own, below, above)
    for i, (m, ref) in enumerate(zip((0, 1, 3), sources)):
        slots_of(spot, cap, planes, slots, m, table_of(ref, rows), pick.at[i], mix.at[i])
    tile = 2 * slots
    for i in range(0, part.shape[0], tile):
        span = pl.ds(i, tile)
        sums = [dot(pick[n, span, :], ref[:rows, :]) for n, ref in enumerate(sources)]
        part[span, :] = (sums[0] + sums[1] + sums[2]).astype(bf16)


def relay_far_kernel(cap, planes, slots, spot, far, part, out, mix, pick):
    rows = pick.shape[1]
    slots_of(spot, cap, planes, slots, 2, table_of(far, rows), pick, mix)
    tile = 2 * slots
    for i in range(0, part.shape[0], tile):
        span = pl.ds(i, tile)
        out[span, :] = part[span, :] + dot(pick[span, :], far[:rows, :]).astype(bf16)


TN = (((0,), (0,)), ((), ()))


def mix_far_kernel(spot, mix, back, far):
    far[...] = lax.dot_general(mix[...], back[...], TN, preferred_element_type=f32).astype(bf16)


def mix_near_kernel(spot, mix, back, own, below, above):
    for i, ref in ((1, below), (2, above), (0, own)):
        sums = lax.dot_general(mix[i], back[...], TN, preferred_element_type=f32)
        ref[...] = sums.astype(ref.dtype)


def body(
    tokens,
    prior_state,
    mix_gain,
    in_weight,
    decay_rate,
    frequency,
    log_step,
    input_map,
    output_map,
    skip_gain,
    out_weight,
    channel_gain,
    expert_gate,
    expert_up,
    expert_down,
    shared_gate,
    shared_up,
    shared_down,
    routes,
    route_weights,
):
    experts, cores = lax.axis_size("ep"), lax.axis_size("tp")
    planes = experts // RING
    spot = lax.axis_index(AXES).astype(jnp.int32).reshape(1)
    seq_rows, top_count = routes.shape
    slot_cap = min(seq_rows, max(2, 3 * seq_rows * top_count // (2 * experts)))
    slots = -(-4 * slot_cap // 8) * 8
    total = NEAR * RING * slots
    width = tokens.shape[1]
    wide = width // 2

    def at(z, x, t):
        return ((z % planes) * RING + x) * cores + t

    everyone = [(z, x, t) for z in range(planes) for x in range(RING) for t in range(cores)]

    def pair(value, shift):
        def mate(z, t):
            up = (z // NEAR + shift + t) % 2 == 0
            return z + NEAR if up else z - NEAR

        return lax.ppermute(
            value, AXES, [(at(z, x, t), at(mate(z, t), x, t)) for z, x, t in everyone]
        )

    def swap(value):
        return lax.ppermute(value, "tp", [(t, cores - 1 - t) for t in range(cores)])

    nearby = [
        [
            at(NEAR * (q - (t if j >= NEAR // 2 else 0)) + j, x, t)
            for j in range(NEAR)
            for x in range(RING)
        ]
        for q in range(planes // NEAR)
        for t in range(cores)
    ]

    def exchange(value):
        tiles = value.reshape(NEAR * RING, slots, value.shape[1])
        tiles = lax.all_to_all(tiles, AXES, 0, 0, axis_index_groups=nearby, tiled=True)
        return tiles.reshape(value.shape)

    table = jnp.concatenate(
        [
            jnp.pad(value.T.astype(bf16), ((0, TABLE - top_count), (0, LANES - seq_rows)))
            for value in (routes, route_weights)
        ],
        axis=1,
    )
    table = jnp.pad(table, ((0, 0), (0, wide - 2 * LANES)))

    lanes = input_map.shape[2]
    imap = input_map.transpose(0, 1, 3, 2).reshape(2, -1, lanes)
    omap = output_map.reshape(2, -1, lanes)
    new_state, partial = mixer(
        tokens,
        mix_gain[None],
        in_weight,
        prior_state,
        decay_rate,
        frequency,
        log_step[None],
        imap,
        omap,
        skip_gain[None],
        out_weight,
    )
    own, other, middle, travel = second_norm(
        spot, tokens, partial, swap(partial), channel_gain[None], table
    )

    below, above = pair(travel, 0), pair(travel, 1)
    far = pair(below, 1)
    shared_part = entry(spot, own, shared_gate, shared_up)
    shared_keep, shared_send = rest(
        spot, shared_part, other, shared_gate, shared_up, shared_down, 0
    )
    shared_recv = swap(shared_send)
    sizes = (slot_cap, planes, slots)
    part, mix_near = call(
        functools.partial(relay_near_kernel, *sizes),
        spot,
        (travel, below, above),
        [((total, wide), bf16), ((3, total, seq_rows), bf16)],
        [pltpu.VMEM((3, total, seq_rows), bf16)],
    )
    part, shared_keep, shared_recv = lax.optimization_barrier((part, shared_keep, shared_recv))
    rows, mix_far = call(
        functools.partial(relay_far_kernel, *sizes),
        spot,
        (far, part),
        [((total, wide), bf16), ((total, seq_rows), bf16)],
        [pltpu.VMEM((total, seq_rows), bf16)],
    )

    arrived = exchange(rows)
    cut = total * 4 // 7
    weights = (expert_gate[0], expert_up[0], expert_down[0])
    others = [swap(arrived[:cut]), swap(arrived[cut:])]
    part = entry(spot, arrived, *weights[:2])
    outs = []
    for other, first in zip(others, (0, cut)):
        outs.append(rest(spot, part, other, *weights, first))
    summed = [keep.astype(f32) + swap(send).astype(f32) for keep, send in outs]
    back = exchange(jnp.concatenate(summed, axis=0).astype(bf16))

    sent, sums = ((seq_rows, wide), bf16), ((seq_rows, wide), f32)
    m_far = call(mix_far_kernel, spot, (mix_far, back), [sent])[0]
    passing = pair(m_far, 0)
    m_own, m_below, m_above = call(mix_near_kernel, spot, (mix_near, back), [sums, sent, sums])
    direct = pair(m_below, 0)
    joined = pair((m_above + passing.astype(f32)).astype(bf16), 1)
    shared_out = shared_keep.astype(f32) + shared_recv.astype(f32)
    known = middle.astype(f32) + shared_out + m_own
    layer_out = (known + direct.astype(f32) + joined.astype(f32)).astype(bf16)
    return (layer_out, new_state)


def solution(mesh):
    in_specs = (
        P(("grp", "ep"), None),
        P(None, ("grp", "ep"), "tp"),
        P(),
        P(None, "tp"),
        P("tp", None),
        P("tp", None),
        P("tp"),
        P(None, "tp", None, None),
        P(None, "tp", None, None),
        P("tp"),
        P("tp", None),
        P(),
        P("ep", None, "tp"),
        P("ep", None, "tp"),
        P("ep", "tp", None),
        P(None, "tp"),
        P(None, "tp"),
        P("tp", None),
        P(("grp", "ep"), None),
        P(("grp", "ep"), None),
    )
    out_specs = (P(("grp", "ep"), "tp"), P(None, ("grp", "ep"), "tp"))
    return jax.shard_map(body, mesh=mesh, in_specs=in_specs, out_specs=out_specs, check_vma=False)
```
